32 devices in a mesh: sp: 8 (over z, x), dp: 4 (over y, core).
Axes of the slice: x: 2, y: 2, z: 4, core: 2. Of those that a mesh axis runs over, the one named last changes fastest.
Arguments:
- hidden_in: bfloat16 [4, 1024, 2048], P('dp', 'sp'), may hold values from -6 to 6
- mix_cotangent: bfloat16 [4, 1024, 4096], P('dp', 'sp'), may hold values from -0.119628906 to 0.119628906
- query_weight: bfloat16 [2048, 4096], P('dp', 'sp'), may hold values from -0.125 to 0.125
- key_weight: bfloat16 [2048, 4096], P('dp', 'sp'), may hold values from -0.125 to 0.125
- value_weight: bfloat16 [2048, 4096], P('dp', 'sp'), may hold values from -0.125 to 0.125
- decay_log: float32 [16], P('sp'), may hold values from -0.034 to -0.00029296875, as said below
Outputs:
- grad_hidden: bfloat16 [4, 1024, 2048], P('dp', 'sp')
- grad_query: float32 [2048, 4096], P('dp', 'sp')
- grad_key: float32 [2048, 4096], P('dp', 'sp')
- grad_value: float32 [2048, 4096], P('dp', 'sp')
The draws below stay inside these ranges and needn't reach their ends.
Inputs may be any that keep to these rules, and one draw needn't show every extreme that they name: Each head's decay_log is negative.
All inputs are finite; a program needn't handle non-finite values.
Results may differ from the reference program's by a relative error of at most 0.015.
Values may be sent and summed in bfloat16 or wider, within the bound.
A program may use at most 64 MiB of HBM per device.

```python
import jax
import jax.numpy as jnp
from jax import lax

D = 2048
HEADS = 16
BLOCK = 128
WIDTH = 4096
SEQ_LEN = 1024
SEQS = 4
N_SP = 8


def draw_decay_log(key, part):
    key_fast = jax.random.fold_in(key, 11)
    key_quick = jax.random.fold_in(key, 12)
    key_slow = jax.random.fold_in(key, 13)
    fast = jax.random.bernoulli(key_fast, 0.5, (HEADS,))
    quick_rate = jax.random.uniform(key_quick, (HEADS,), jnp.float32, 0.01, 0.034)
    slow_rate = jax.random.uniform(key_slow, (HEADS,), jnp.float32, 0.3, 2.0) / SEQ_LEN
    return -jnp.where(fast, quick_rate, slow_rate).astype(jnp.float32)


def block_levels(own_key, extent, cuts, smallest, largest):
    gain = 1.0
    for position, parts in cuts:
        heights = jax.random.uniform(jax.random.fold_in(jax.random.fold_in(own_key, 6), position), (parts,), jnp.float32, smallest / len(cuts), largest / len(cuts))
        gain = gain * jnp.repeat(jnp.exp(heights), extent[position] // parts).reshape((-1,) + (1,) * (len(extent) - 1 - position))
    return gain


def noise(rng, extent, scale, reach, split=(), kind=jnp.bfloat16):
    array = scale * jax.random.normal(rng, extent, jnp.float32)
    if split:
        array = array * block_levels(rng, extent, split, -0.22, 0.18)
    return jnp.clip(array, -reach, reach).astype(kind)


def setup_inputs(seed: int = 0) -> dict:
    seeds = jax.random.split(jax.random.key(seed), 7)
    return {
        "hidden_in": noise(seeds[0], (SEQS, SEQ_LEN, D), 1.0, 6.0, ((0, 4), (1, 8))),
        "mix_cotangent": noise(seeds[1], (SEQS, SEQ_LEN, WIDTH), 0.02, 0.119628906, ((0, 4), (1, 8))),
        "query_weight": noise(seeds[2], (D, WIDTH), D ** -0.5, 0.125, ((0, 4), (1, 8))),
        "key_weight": noise(seeds[3], (D, WIDTH), D ** -0.5, 0.125, ((0, 4), (1, 8))),
        "value_weight": noise(seeds[4], (D, WIDTH), D ** -0.5, 0.125, ((0, 4), (1, 8))),
        "decay_log": draw_decay_log(jax.random.fold_in(seeds[6], 71), 0),
    }


def head_grads(queries, key_rows, values, cotangent, log_rate):
    length = queries.shape[0]
    head_dim = queries.shape[1]
    blocks = length // BLOCK
    scale = head_dim ** -0.5
    keys_scaled = (key_rows.astype(jnp.float32) * scale).astype(jnp.bfloat16)
    offsets = jnp.arange(BLOCK, dtype=jnp.float32)
    spread = offsets[:, None] - offsets[None, :]
    inner_decay = jnp.where(spread >= 0, jnp.exp(log_rate * jnp.maximum(spread, 0.0)), 0.0)
    query_decay = jnp.exp(log_rate * (offsets + 1.0))
    key_decay = jnp.exp(log_rate * (BLOCK - 1.0 - offsets))
    block_decay = jnp.exp(log_rate * BLOCK)

    def split_blocks(series):
        return series.reshape(blocks, BLOCK, series.shape[-1])

    def forward(carried, inputs):
        query_block, key_block, value_block, grad_block = inputs
        mixed = (jnp.dot(grad_block, value_block.T, preferred_element_type=jnp.float32) * inner_decay).astype(jnp.bfloat16)
        within = jnp.dot(mixed, key_block, preferred_element_type=jnp.float32)
        across = jnp.dot(grad_block, carried.astype(jnp.bfloat16).T, preferred_element_type=jnp.float32) * query_decay[:, None]
        weighted = (key_block.astype(jnp.float32) * key_decay[:, None]).astype(jnp.bfloat16)
        updated = carried * block_decay + jnp.dot(weighted.T, value_block, preferred_element_type=jnp.float32)
        return updated, (within + across, mixed)

    def backward(carried, inputs):
        query_block, key_block, value_block, grad_block, mixed = inputs
        scores = (jnp.dot(query_block, key_block.T, preferred_element_type=jnp.float32) * inner_decay).astype(jnp.bfloat16)
        state_bf = carried.astype(jnp.bfloat16)
        grad_v = jnp.dot(scores.T, grad_block, preferred_element_type=jnp.float32) + jnp.dot(key_block, state_bf, preferred_element_type=jnp.float32) * key_decay[:, None]
        grad_k = (jnp.dot(mixed.T, query_block, preferred_element_type=jnp.float32) + jnp.dot(value_block, state_bf.T, preferred_element_type=jnp.float32) * key_decay[:, None]) * scale
        weighted = (query_block.astype(jnp.float32) * query_decay[:, None]).astype(jnp.bfloat16)
        updated = carried * block_decay + jnp.dot(weighted.T, grad_block, preferred_element_type=jnp.float32)
        return updated, (grad_k, grad_v)

    inputs = (split_blocks(queries), split_blocks(keys_scaled), split_blocks(values), split_blocks(cotangent))
    initial = jnp.zeros((head_dim, values.shape[-1]), jnp.float32)
    final_state, (grad_q, mixed_all) = lax.scan(forward, initial, inputs)
    final_back, (grad_k, grad_v) = lax.scan(backward, initial, inputs + (mixed_all,), reverse=True)
    return grad_q.reshape(length, -1), grad_k.reshape(length, -1), grad_v.reshape(length, -1)


def group_grads(log_rates, queries, key_rows, values, cotangent):
    length = queries.shape[0]
    head_count = log_rates.shape[0]

    def by_head(series):
        return series.reshape(length, head_count, -1).transpose(1, 0, 2)

    def to_rows(series):
        return series.transpose(1, 0, 2).reshape(length, -1)

    grad_q, grad_k, grad_v = jax.vmap(head_grads)(by_head(queries), by_head(key_rows), by_head(values), by_head(cotangent), log_rates)
    return jnp.concatenate((to_rows(grad_q), to_rows(grad_k), to_rows(grad_v)), axis=1).astype(jnp.bfloat16)


def reference(hidden_in, mix_cotangent, query_weight, key_weight, value_weight, decay_log):
    weights = jnp.concatenate((query_weight, key_weight, value_weight), axis=1)
    all_width = query_weight.shape[1]
    model_width = query_weight.shape[0]

    def one_sequence(seq_pair):
        seq_rows, seq_cotangent = seq_pair
        projected = jnp.dot(seq_rows, weights, preferred_element_type=jnp.float32).astype(jnp.bfloat16)
        gradients = group_grads(decay_log, projected[:, :all_width], projected[:, all_width:2 * all_width], projected[:, 2 * all_width:], seq_cotangent)
        length = seq_rows.shape[0]
        split_grads = gradients.reshape(length, 3, N_SP, -1).astype(jnp.float32)
        split_weights = weights.reshape(model_width, 3, N_SP, -1).astype(jnp.float32)
        partials = jnp.einsum('ltgc,dtgc->gld', split_grads, split_weights)
        rounded = lax.optimization_barrier(partials.astype(jnp.bfloat16)).astype(jnp.float32)
        return jnp.sum(rounded, axis=0).astype(jnp.bfloat16), gradients

    grad_hidden, all_grads = lax.map(one_sequence, (hidden_in, mix_cotangent))
    flat_rows = hidden_in.reshape(-1, model_width)
    flat_grads = all_grads.reshape(-1, 3 * all_width)
    summed = lax.dot_general(flat_rows, flat_grads, (((0,), (0,)), ((), ())), preferred_element_type=jnp.float32) / SEQS
    return grad_hidden, summed[:, :all_width], summed[:, all_width:2 * all_width], summed[:, 2 * all_width:]
```

```python
import functools

import jax
import jax.numpy as jnp
from jax import lax
from jax.experimental import pallas as pl
from jax.experimental.pallas import tpu as pltpu
from jax.sharding import PartitionSpec as P

BLOCK = 128
SUBS = 2
CHUNKS = 4
PIECES = 4
F32 = jnp.float32
BF16 = jnp.bfloat16
MESH = pl.DeviceIdType.MESH
NT = (((1,), (1,)), ((), ()))
TN = (((0,), (0,)), ((), ()))
VMEM_LIMIT = 52 * 1024 * 1024


def dot(a, b, dims=(((1,), (0,)), ((), ()))):
    return lax.dot_general(a, b, dims, preferred_element_type=F32)


def scope(name, *tags):
    return jax.named_scope("#".join([name] + [str(t) for t in tags]))


def remote(src, dst, send, recv, where):
    return pltpu.make_async_remote_copy(
        src_ref=src, dst_ref=dst, send_sem=send, recv_sem=recv, device_id=where, device_id_type=MESH
    )


def greet(targets):
    barrier = pltpu.get_barrier_semaphore()
    for where in targets:
        pl.semaphore_signal(barrier, inc=1, device_id=where, device_id_type=MESH)
    return lambda: pl.semaphore_wait(barrier, len(targets))


def gather_phase(
    n, m, project, h_in, c_in, wq, wk, wv, h_all, c_all, w_all, c_own, l_sem,
    h_recv, h_line, h_side, c_send, c_recv, w_far, w_near, w_recv,
):
    s = lax.axis_index("sp")
    d = lax.axis_index("dp")
    z, x = s // 2, s % 2
    y, core = d // 2, d % 2
    nz, ny = n // 2, m // 2
    rows = h_in.shape[0]
    sub_rows = rows // SUBS
    depth, columns = wq.shape
    side = s + 1 - 2 * x
    mate = d + 1 - 2 * core

    def far(o):
        return ((y + o) % ny) * 2 + core

    arrived = greet(
        [{"sp": (s + k) % n} for k in range(1, n)]
        + [{"dp": mate}]
        + [{"dp": far(o)} for o in range(1, ny)]
    )

    own_rows = pl.ds(pl.multiple_of(s * rows, rows), rows)
    own_depth = pl.ds(pl.multiple_of(d * depth, depth), depth)
    loads = [pltpu.make_async_copy(h_in, h_all.at[own_rows], l_sem.at[0])]
    for j, w in enumerate((wq, wk, wv)):
        place = w_all.at[own_depth, pl.ds(j * columns, columns)]
        loads.append(pltpu.make_async_copy(w, place, l_sem.at[1 + j]))
    loads.append(pltpu.make_async_copy(c_in, c_own, l_sem.at[4]))
    mine = c_in.at[:, pl.ds(pl.multiple_of(s * columns, columns), columns)]
    loads.append(pltpu.make_async_copy(mine, c_all.at[own_rows], l_sem.at[5]))
    for load in loads:
        load.start()

    def h_copy(src_z, src_x, sub, dest, send):
        block = src_z * 2 + src_x
        place = pl.ds(pl.multiple_of(block * rows + sub * sub_rows, sub_rows), sub_rows)
        return remote(h_all.at[place], h_all.at[place], send, h_recv.at[block, sub], {"sp": dest})

    def w_copy(src_d, j, dest, send):
        place = w_all.at[
            pl.ds(pl.multiple_of(src_d * depth, depth), depth), pl.ds(j * columns, columns)
        ]
        return remote(place, place, send, w_recv.at[src_d, j], {"dp": dest})

    def c_copy(k):
        to = (s + k) % n
        return remote(
            c_own.at[:, pl.ds(pl.multiple_of(to * columns, columns), columns)],
            c_all.at[pl.ds(pl.multiple_of(s * rows, rows), rows)],
            c_send.at[k - 1],
            c_recv.at[k - 1],
            {"sp": to},
        )

    def line(k, sub, up):
        source = (z - k) if up else (z + k)
        dest = (s + 2) if up else (s - 2)
        return h_copy(source, x, sub, dest, h_line.at[k, sub, int(up)])

    def goes(k, up):
        if up:
            return jnp.logical_and(z - k >= 0, z + 1 < nz)
        return jnp.logical_and(z + k < nz, z >= 1)

    def arrives(k, up):
        return (z - k >= 0) if up else (z + k < nz)

    with scope("greet"):
        loads[0].wait()
        arrived()
    for sub in range(SUBS):
        for up in (True, False):

            @pl.when(goes(0, up))
            def _():
                line(0, sub, up).start()

        h_copy(z, x, sub, side, h_side.at[0, sub, 0]).start()
    for j in range(3):
        loads[1 + j].wait()
        for o in range(1, ny):
            w_copy(d, j, far(o), w_far.at[o, j]).start()
        w_copy(d, j, mate, w_near.at[0, j]).start()
    loads[4].wait()
    loads[5].wait()

    def pass_weights(j):
        for o in range(1, ny):
            with scope("wfar", j):
                w_copy(far(o), j, mate, w_near.at[o, j]).wait_recv()
            w_copy(far(o), j, mate, w_near.at[o, j]).start()

    def send_cotangent():
        for hop in range(1, n):
            c_copy(hop).start()

    passed = 0
    for k in range(1, nz):
        for sub in range(SUBS):
            for up in (True, False):

                @pl.when(arrives(k, up))
                def _():
                    source = (z - k) if up else (z + k)
                    with scope("hline", k, sub, up):
                        h_copy(source, x, sub, side, h_side.at[k, sub, int(up)]).wait_recv()
                    h_copy(source, x, sub, side, h_side.at[k, sub, int(up)]).start()

                @pl.when(goes(k, up))
                def _():
                    line(k, sub, up).start()

    send_cotangent()
    for j in range(passed, 3):
        pass_weights(j)

    for j in range(3):
        w_copy(mate, j, mate, w_near.at[0, j]).wait_recv()
        for o in range(1, ny):
            other = far(o) + 1 - 2 * core
            with scope("wmate", j):
                w_copy(other, j, mate, w_near.at[o, j]).wait_recv()

    @pl.loop(0, nz)
    def _(zz):
        with scope("projown"):
            project(zz * 2 + x)

    turn = 1 - 2 * (z // ((nz + 1) // 2))

    @pl.loop(0, nz)
    def _(k):
        zz = (z + turn * k + nz) % nz
        with scope("sidewait"):
            for sub in range(SUBS):
                h_copy(zz, 1 - x, sub, side, h_side.at[0, sub, 0]).wait_recv()
        with scope("projside"):
            project(zz * 2 + 1 - x)

    with scope("cwait"):
        for k in range(1, n):
            c_copy(k).wait_recv()

    def drain():
        for k in range(1, n):
            c_copy(k).wait_send()
        for j in range(3):
            for o in range(ny):
                w_copy(d, j, mate, w_near.at[o, j]).wait_send()
                if o:
                    w_copy(d, j, far(o), w_far.at[o, j]).wait_send()
        for sub in range(SUBS):
            h_copy(z, x, sub, side, h_side.at[0, sub, 0]).wait_send()
            for up in (True, False):
                for k in range(nz):

                    @pl.when(goes(k, up))
                    def _():
                        line(k, sub, up).wait_send()

                    if k:

                        @pl.when(arrives(k, up))
                        def _():
                            h_copy(z, x, sub, side, h_side.at[k, sub, int(up)]).wait_send()

    return drain


def project_block(h_all, w_all, p_all, rows, columns, scale, block):
    at = pl.ds(pl.multiple_of(block * rows, rows), rows)
    for j in range(3):
        value = dot(h_all[at, :], w_all[:, j * columns : (j + 1) * columns]).astype(BF16)
        if j == 1:
            value = (value.astype(F32) * scale).astype(BF16)
        p_all[at, j * columns : (j + 1) * columns] = value


def mixer_phase(heads, rate, c_all, p_all, g_all, state, back):
    length, columns = c_all.shape
    dim = columns // heads
    blocks = length // BLOCK
    scale = dim ** (-0.5)
    row = lax.broadcasted_iota(jnp.int32, (BLOCK, BLOCK), 0).astype(F32)
    col = lax.broadcasted_iota(jnp.int32, (BLOCK, BLOCK), 1).astype(F32)
    place = lax.broadcasted_iota(jnp.int32, (BLOCK, dim), 0).astype(F32)
    spread = row - col
    state[...] = jnp.zeros_like(state)
    back[...] = jnp.zeros_like(back)

    @pl.loop(0, blocks)
    def _(i):
        for h in range(heads):
            g = rate[h]
            inner = jnp.where(spread >= 0, jnp.exp(g * jnp.maximum(spread, 0.0)), 0.0)
            inner_t = jnp.where(spread <= 0, jnp.exp(g * jnp.maximum(-spread, 0.0)), 0.0)
            query_decay = jnp.exp(g * (place + 1.0))
            key_decay = jnp.exp(g * (BLOCK - 1.0 - place))
            block_decay = jnp.exp(jnp.full((1, dim), g * BLOCK, F32))
            parts = [slice(j * columns + h * dim, j * columns + (h + 1) * dim) for j in range(3)]

            at = pl.ds(pl.multiple_of(i * BLOCK, BLOCK), BLOCK)
            k, v = p_all[at, parts[1]], p_all[at, parts[2]]
            c = c_all[at, parts[0]]
            mixed = (dot(c, v, NT) * inner).astype(BF16)
            held = state[h]
            grad_q = dot(mixed, k) + dot(c, held.astype(BF16), NT) * query_decay
            weighted = (k.astype(F32) * key_decay).astype(BF16)
            state[h] = held * block_decay + dot(weighted, v, TN)
            g_all[at, parts[0]] = grad_q.astype(BF16)

            at = pl.ds(pl.multiple_of((blocks - 1 - i) * BLOCK, BLOCK), BLOCK)
            q, k, v = (p_all[at, part] for part in parts)
            c = c_all[at, parts[0]]
            mixed_t = (dot(v, c, NT) * inner_t).astype(BF16)
            scores_t = (dot(k, q, NT) * inner_t).astype(BF16)
            held = back[h]
            held_bf = held.astype(BF16)
            grad_v = dot(scores_t, c) + dot(k, held_bf) * key_decay
            grad_k = (dot(mixed_t, q) + dot(v, held_bf, NT) * key_decay) * scale
            weighted = (q.astype(F32) * query_decay).astype(BF16)
            back[h] = held * block_decay + dot(weighted, c, TN)
            g_all[at, parts[1]] = grad_k.astype(BF16)
            g_all[at, parts[2]] = grad_v.astype(BF16)


def scatter_phase(
    n, m, h_all, w_all, g_all, dh, dq, dk, dv,
    part, ring, turned, near_out, near_in, far_out, far_in,
    r_send, r_recv, n_send, n_recv, f_send, f_recv,
):
    s = lax.axis_index("sp")
    d = lax.axis_index("dp")
    z, x = s // 2, s % 2
    y, core = d // 2, d % 2
    nz, ny = n // 2, m // 2
    rows, width = dh.shape
    depth, columns = dq.shape
    chunk = width // CHUNKS
    lanes = rows // 2
    mate = d + 1 - 2 * core
    me = x * (n - 1 - z) + (1 - x) * z

    def at_ring(p):
        p = (p + 2 * n) % n
        hi = p // nz
        return (hi * (n - 1 - p) + (1 - hi) * p) * 2 + hi

    def far(o):
        return ((y + o) % ny) * 2 + core

    right, left = at_ring(me + 1), at_ring(me - 1)

    def own(offset):
        return pl.multiple_of(at_ring(me + offset) * rows, rows)

    ready = set()

    def partial(q, *offsets):
        todo = [o % n for o in offsets if (q, o % n) not in ready]
        if not todo:
            return
        ready.update((q, o) for o in todo)
        bases = [own(o) for o in todo]
        with scope("partial", q, *todo):
            lhs = jnp.concatenate([g_all[pl.ds(base, rows), :] for base in bases], axis=0)
            value = dot(lhs, w_all[q * chunk : (q + 1) * chunk, :], NT).astype(BF16)
            for place, base in enumerate(bases):
                part[q, pl.ds(base, rows), :] = value[place * rows : (place + 1) * rows]

    def spot(way, piece):
        return way * (CHUNKS // 2) + piece // 2, (piece % 2) * lanes

    def r_copy(step, way, piece):
        q, lane = spot(way, piece)
        if step == 0:
            base = own(-1 if way == 0 else 1)
            src = part.at[q, pl.ds(pl.multiple_of(base + lane, lanes), lanes)]
        else:
            src = ring.at[step - 1, way, piece]
        return remote(
            src,
            ring.at[step, way, piece],
            r_send.at[step, way, piece],
            r_recv.at[step, way, piece],
            {"sp": right if way == 0 else left},
        )

    def process(step, piece):
        for way in range(2):
            offset = -(step + 2) if way == 0 else step + 2
            q, lane = spot(way, piece)
            partial(q, -(step + 2), step + 2)
            with scope("ring", step, way, piece):
                r_copy(step, way, piece).wait_recv()
            mine = part[q, pl.ds(pl.multiple_of(own(offset) + lane, lanes), lanes), :]
            total = (ring[step, way, piece].astype(F32) + mine.astype(F32)).astype(BF16)
            if step < n - 2:
                ring[step, way, piece] = total
                r_copy(step + 1, way, piece).start()
            else:
                dh[lane : lane + lanes, q * chunk : (q + 1) * chunk] = total

    def turn(slot, device):
        turned[slot] = h_all[:, pl.ds(pl.multiple_of(device * depth, depth), depth)].T

    def weight_part(slot, j):
        return dot(turned[slot], g_all[:, j * columns : (j + 1) * columns])

    def n_copy(o, j):
        return remote(
            near_out.at[o, j], near_in.at[o, j], n_send.at[o, j], n_recv.at[o, j], {"dp": mate}
        )

    def f_copy(o, j):
        return remote(
            far_out.at[o - 1, j], far_in.at[o - 1, j], f_send.at[o - 1, j], f_recv.at[o - 1, j], {"dp": far(o)}
        )

    def near(o, j):
        if j == 0:
            turn(0, far(o) + 1 - 2 * core)
        with scope("near", o, j):
            near_out[o, j] = weight_part(0, j).astype(BF16)
        n_copy(o, j).start()

    def chip_sum(o, j):
        if j == 0:
            turn(1, far(o))
        with scope("chip_sum", o, j):
            value = weight_part(1, j)
            n_copy(o, j).wait_recv()
            value = value + near_in[o, j].astype(F32)
        if o:
            far_out[o - 1, j] = value.astype(BF16)
            f_copy(o, j).start()
        else:
            (dq, dk, dv)[j][...] = value

    def weight(kind, o, j):
        return functools.partial(kind, o, j)

    tasks = []
    for o in list(range(1, ny)) + [0]:
        tasks += [weight(near, o, 0), weight(near, o, 1), weight(chip_sum, o, 0)]
        tasks += [weight(near, o, 2), weight(chip_sum, o, 1), weight(chip_sum, o, 2)]

    def work(count=1):
        for _ in range(count):
            if tasks:
                tasks.pop(0)()

    order = [q for k in range(CHUNKS // 2) for q in (k, CHUNKS // 2 + k)]
    for q in order:
        partial(q, -1, 1)
        way, first = divmod(q, CHUNKS // 2)
        for piece in (2 * first, 2 * first + 1):
            r_copy(0, way, piece).start()
    work()
    for q in order[:2]:
        partial(q, -2, 2)
    work(2)
    pairs = [(q, pair) for pair in [(-2, 2), (-3, 3), (n // 2, 0)] for q in order]
    for step in range(n - 1):
        for piece in range(PIECES):
            process(step, piece)
            while pairs and all((pairs[0][0], o % n) in ready for o in pairs[0][1]):
                pairs.pop(0)
            if pairs and (step < 2 or not tasks):
                q, pair = pairs.pop(0)
                partial(q, *pair)
                if step and piece % 2:
                    work()
            else:
                work()
    work(len(tasks))
    for j, out in enumerate((dq, dk, dv)):
        total = out[...]
        for o in range(1, ny):
            with scope("fwait", o, j):
                f_copy(o, j).wait_recv()
            total = total + far_in[o - 1, j].astype(F32)
        out[...] = total * (1.0 / m)
    for step in range(n - 1):
        for piece in range(PIECES):
            for way in range(2):
                r_copy(step, way, piece).wait_send()
    for o in range(ny):
        for j in range(3):
            n_copy(o, j).wait_send()
            if o:
                f_copy(o, j).wait_send()


def whole_kernel(n, m, heads, rate, h_in, c_in, wq, wk, wv, dh, dq, dk, dv, *scratch):
    h_all, c_all, w_all, p_all, g_all, state, back = scratch[:7]
    gather_sems, rest = scratch[7:17], scratch[17:]
    columns = wq.shape[1]
    project = functools.partial(
        project_block, h_all, w_all, p_all, h_in.shape[0], columns, (columns // heads) ** (-0.5)
    )
    drain = gather_phase(
        n, m, project, h_in, c_in, wq, wk, wv, h_all, c_all, w_all, *gather_sems
    )
    with scope("mixer"):
        mixer_phase(heads, rate, c_all, p_all, g_all, state, back)
    scatter_phase(n, m, h_all, w_all, g_all, dh, dq, dk, dv, *rest)
    with scope("drain"):
        drain()


def whole(n, m, rate, h, c, wq, wk, wv):
    rows, width = h.shape
    depth, columns = wq.shape
    heads = rate.shape[0]
    dim = columns // heads
    length = rows * n
    ny = m // 2
    vmem = pl.BlockSpec(memory_space=pltpu.VMEM)
    dma = pltpu.SemaphoreType.DMA
    return pl.pallas_call(
        functools.partial(whole_kernel, n, m, heads),
        out_shape=(pltpu.VMEM((rows, width), BF16),)
        + (pltpu.VMEM((depth, columns), F32),) * 3,
        in_specs=[pl.BlockSpec(memory_space=pltpu.SMEM)]
        + [pl.BlockSpec(memory_space=pl.ANY)] * 5,
        out_specs=(vmem,) * 4,
        scratch_shapes=[
            pltpu.VMEM((length, width), BF16),
            pltpu.VMEM((length, columns), BF16),
            pltpu.VMEM((depth * m, 3 * columns), BF16),
            pltpu.VMEM((length, 3 * columns), BF16),
            pltpu.VMEM((length, 3 * columns), BF16),
            pltpu.VMEM((heads, dim, dim), F32),
            pltpu.VMEM((heads, dim, dim), F32),
            pltpu.VMEM((rows, columns * n), BF16),
            dma((6,)),
            dma((n, SUBS)),
            dma((n // 2, SUBS, 2)),
            dma((n // 2, SUBS, 2)),
            dma((n - 1,)),
            dma((n - 1,)),
            dma((ny, 3)),
            dma((ny, 3)),
            dma((m, 3)),
            pltpu.VMEM((CHUNKS, length, width // CHUNKS), BF16),
            pltpu.VMEM((n - 1, 2, PIECES, rows // 2, width // CHUNKS), BF16),
            pltpu.VMEM((2, depth, length), BF16),
            pltpu.VMEM((ny, 3, depth, columns), BF16),
            pltpu.VMEM((ny, 3, depth, columns), BF16),
            pltpu.VMEM((ny - 1, 3, depth, columns), BF16),
            pltpu.VMEM((ny - 1, 3, depth, columns), BF16),
            dma((n - 1, 2, PIECES)),
            dma((n - 1, 2, PIECES)),
            dma((ny, 3)),
            dma((ny, 3)),
            dma((ny - 1, 3)),
            dma((ny - 1, 3)),
        ],
        compiler_params=pltpu.CompilerParams(
            collective_id=0, has_side_effects=True, vmem_limit_bytes=VMEM_LIMIT
        ),
        name="whole",
    )(rate, h, c, wq, wk, wv)


def finish_kernel(count, *refs):
    ins, outs, sems = refs[:count], refs[count : 2 * count], refs[2 * count]
    moves = [pltpu.make_async_copy(ins[i], outs[i], sems.at[i]) for i in range(count)]
    for move in moves:
        move.start()
    for move in moves:
        move.wait()


def finish(*arrays):
    count = len(arrays)
    return pl.pallas_call(
        functools.partial(finish_kernel, count),
        out_shape=tuple(jax.ShapeDtypeStruct(a.shape, a.dtype) for a in arrays),
        in_specs=[pl.BlockSpec(memory_space=pltpu.VMEM)] * count,
        out_specs=(pl.BlockSpec(memory_space=pl.ANY),) * count,
        scratch_shapes=[pltpu.SemaphoreType.DMA((count,))],
        compiler_params=pltpu.CompilerParams(vmem_limit_bytes=4 * 1024 * 1024),
        name="finish",
    )(*arrays)


def body(n, m, hidden_in, mix_cotangent, query_weight, key_weight, value_weight, decay_log):
    dh, dq, dk, dv = finish(
        *whole(
            n, m, decay_log, hidden_in[0], mix_cotangent[0], query_weight, key_weight, value_weight
        )
    )
    return dh[None], dq, dk, dv


def solution(mesh):
    placed = (
        P("dp", "sp", None),
        P("dp", "sp", None),
        P("dp", "sp"),
        P("dp", "sp"),
        P("dp", "sp"),
        P("sp"),
    )
    return jax.shard_map(
        functools.partial(body, mesh.shape["sp"], mesh.shape["dp"]),
        mesh=mesh,
        in_specs=placed,
        out_specs=(P("dp", "sp", None), P("dp", "sp"), P("dp", "sp"), P("dp", "sp")),
        check_vma=False,
    )
```

```python
import functools

import jax
import jax.numpy as jnp
from jax import lax
from jax.experimental import pallas as pl
from jax.experimental.pallas import tpu as pltpu
from jax.sharding import PartitionSpec as P

BLOCK = 128
SUBS = 2
CHUNKS = 4
PIECES = 4
F32 = jnp.float32
BF16 = jnp.bfloat16
MESH = pl.DeviceIdType.MESH
NT = (((1,), (1,)), ((), ()))
TN = (((0,), (0,)), ((), ()))
VMEM_LIMIT = 58 * 1024 * 1024


def dot(a, b, dims=(((1,), (0,)), ((), ()))):
    return lax.dot_general(a, b, dims, preferred_element_type=F32)


def scope(name, *tags):
    return jax.named_scope("#".join([name] + [str(t) for t in tags]))


def remote(src, dst, send, recv, where):
    return pltpu.make_async_remote_copy(
        src_ref=src, dst_ref=dst, send_sem=send, recv_sem=recv, device_id=where, device_id_type=MESH
    )


def greet(always, sometimes):
    barrier = pltpu.get_barrier_semaphore()
    count = len(always)
    for where in always:
        pl.semaphore_signal(barrier, inc=1, device_id=where, device_id_type=MESH)
    for there, where in sometimes:
        count = count + jnp.where(there, 1, 0)

        @pl.when(there)
        def _():
            pl.semaphore_signal(barrier, inc=1, device_id=where, device_id_type=MESH)

    return lambda: pl.semaphore_wait(barrier, count)


def gather_phase(
    n, m, project, local, tables, h_in, c_in, wq, wk, wv, h_all, c_all, w_all, c_own, c_via, l_sem,
    h_recv, h_line, h_side, h_bridge, c_send, c_recv, v_send, v_recv, w_far, w_near, w_recv,
):
    s = lax.axis_index("sp")
    d = lax.axis_index("dp")
    z, x = s // 2, s % 2
    y, core = d // 2, d % 2
    nz, ny = n // 2, m // 2
    rows = h_in.shape[0]
    sub_rows = rows // SUBS
    depth, columns = wq.shape
    side = s + 1 - 2 * x
    mate = d + 1 - 2 * core
    bridged = nz > 2
    is_end = jnp.logical_or(z == 0, z == nz - 1)
    inner = jnp.logical_not(is_end)
    inward = jnp.where(z == 0, s + 2, s - 2)

    def far(o):
        return ((y + o) % ny) * 2 + core

    arrived = greet(
        [{"sp": side}, {"dp": mate}] + [{"dp": far(o)} for o in range(1, ny)],
        [(z >= 1, {"sp": s - 2}), (z + 1 < nz, {"sp": s + 2})],
    )

    def part_rows(block):
        return pl.ds(pl.multiple_of(block * rows, rows), rows)

    def part_columns(block):
        return pl.ds(pl.multiple_of(block * columns, columns), columns)

    own_depth = pl.ds(pl.multiple_of(d * depth, depth), depth)
    loads = [pltpu.make_async_copy(h_in, h_all.at[part_rows(s)], l_sem.at[0])]
    for j, w in enumerate((wq, wk, wv)):
        place = w_all.at[own_depth, pl.ds(j * columns, columns)]
        loads.append(pltpu.make_async_copy(w, place, l_sem.at[1 + j]))
    loads.append(pltpu.make_async_copy(c_in, c_own, l_sem.at[4]))
    mine = c_in.at[:, part_columns(s)]
    loads.append(pltpu.make_async_copy(mine, c_all.at[part_rows(s)], l_sem.at[5]))
    for load in loads:
        load.start()

    def h_copy(src_z, src_x, sub, dest, send):
        block = src_z * 2 + src_x
        place = pl.ds(pl.multiple_of(block * rows + sub * sub_rows, sub_rows), sub_rows)
        return remote(h_all.at[place], h_all.at[place], send, h_recv.at[block, sub], {"sp": dest})

    def w_copy(src_d, j, dest, send):
        place = w_all.at[
            pl.ds(pl.multiple_of(src_d * depth, depth), depth), pl.ds(j * columns, columns)
        ]
        return remote(place, place, send, w_recv.at[src_d, j], {"dp": dest})

    def c_copy(to):
        return remote(
            c_own.at[:, part_columns(to)], c_all.at[part_rows(s)], c_send.at[to], c_recv.at[s], {"sp": to}
        )

    def c_arrival(block):
        return remote(
            c_all.at[part_rows(block)], c_all.at[part_rows(block)], c_send.at[block], c_recv.at[block], {"sp": side}
        )

    def end_block(e, column):
        return e * (nz - 1) * 2 + column

    def c_cross(e):
        to = end_block(e, 1 - x)
        return remote(
            c_own.at[:, part_columns(to)], c_via.at[e], c_send.at[to], v_recv.at[e], {"sp": side}
        )

    def c_pass(e):
        return remote(
            c_via.at[e], c_all.at[part_rows(side)], v_send.at[e], c_recv.at[side], {"sp": end_block(e, x)}
        )

    def line(k, sub, up):
        source = (z - k) if up else (z + k)
        dest = (s + 2) if up else (s - 2)
        return h_copy(source, x, sub, dest, h_line.at[k, sub, int(up)])

    def goes(k, up):
        if up:
            return jnp.logical_and(z - k >= 0, z + 1 < nz)
        return jnp.logical_and(z + k < nz, z >= 1)

    def arrives(k, up):
        return (z - k >= 0) if up else (z + k < nz)

    def crosses(k, up):
        here = arrives(k, up)
        if not bridged or k != 1:
            return here
        return jnp.logical_and(here, (z != 1) if up else (z != nz - 2))

    def bridge(sub):
        return h_copy(z, 1 - x, sub, inward, h_bridge.at[sub])

    with scope("greet"):
        loads[0].wait()
        arrived()
    for sub in range(SUBS):
        for up in (True, False):

            @pl.when(goes(0, up))
            def _():
                line(0, sub, up).start()

        h_copy(z, x, sub, side, h_side.at[0, sub, 0]).start()
    for j in range(3):
        loads[1 + j].wait()
        for o in range(1, ny):
            w_copy(d, j, far(o), w_far.at[o, j]).start()
        w_copy(d, j, mate, w_near.at[0, j]).start()
    loads[4].wait()
    loads[5].wait()
    if bridged:

        @pl.when(inner)
        def _():
            for e in range(2):
                c_cross(e).start()

    tables()

    def pass_weights(j):
        for o in range(1, ny):
            with scope("wfar", j):
                w_copy(far(o), j, mate, w_near.at[o, j]).wait_recv()
            w_copy(far(o), j, mate, w_near.at[o, j]).start()

    def send_level(k, columns_too):
        for up in (True, False):
            to_z = (z + k) if up else (z - k)

            @pl.when((to_z < nz) if up else (to_z >= 0))
            def _():
                c_copy(to_z * 2 + x).start()
                if columns_too:
                    c_copy(to_z * 2 + 1 - x).start()

    def send_inner():
        c_copy(side).start()
        for k in range(1, nz):
            for up in (True, False):
                to_z = (z + k) if up else (z - k)

                @pl.when((to_z < nz) if up else (to_z >= 0))
                def _():
                    c_copy(to_z * 2 + x).start()

                @pl.when((to_z < nz - 1) if up else (to_z >= 1))
                def _():
                    c_copy(to_z * 2 + 1 - x).start()

                @pl.when(to_z == (nz - 1 if up else 0))
                def _():
                    c_cross(int(up)).wait_recv()
                    c_pass(int(up)).start()

    passed = 0
    for k in range(1, nz):
        if bridged and k == nz - 1:

            @pl.when(inner)
            def _():
                send_inner()

        for sub in range(SUBS):
            for up in (True, False):

                @pl.when(arrives(k, up))
                def _():
                    source = (z - k) if up else (z + k)
                    with scope("hline", k, sub, up):
                        h_copy(source, x, sub, side, h_side.at[k, sub, int(up)]).wait_recv()

                @pl.when(crosses(k, up))
                def _():
                    source = (z - k) if up else (z + k)
                    h_copy(source, x, sub, side, h_side.at[k, sub, int(up)]).start()

                @pl.when(goes(k, up))
                def _():
                    line(k, sub, up).start()

            if bridged and k == 1:

                @pl.when(is_end)
                def _():
                    h_copy(z, 1 - x, sub, side, h_side.at[0, sub, 0]).wait_recv()
                    bridge(sub).start()

            if bridged and (k, sub) in ((nz - 2, 0), (nz - 2, SUBS - 1), (nz - 1, 0)):
                pass_weights(passed)
                passed += 1
        if bridged:

            @pl.when(is_end)
            def _():
                if k == 1:
                    c_copy(side).start()
                send_level(k, True)

    if not bridged:
        c_copy(side).start()
        for k in range(1, nz):
            send_level(k, True)

    for j in range(passed, 3):
        pass_weights(j)

    for j in range(3):
        w_copy(mate, j, mate, w_near.at[0, j]).wait_recv()
        for o in range(1, ny):
            other = far(o) + 1 - 2 * core
            with scope("wmate", j):
                w_copy(other, j, mate, w_near.at[o, j]).wait_recv()

    turn = 1 - 2 * (z // ((nz + 1) // 2))

    def level(k):
        return (z + turn * k + nz) % nz

    def project_side(zz):
        fresh = jnp.logical_not(jnp.logical_and(is_end, zz == z)) if bridged else True
        with scope("sidewait"):

            @pl.when(fresh)
            def _():
                for sub in range(SUBS):
                    h_copy(zz, 1 - x, sub, side, h_side.at[0, sub, 0]).wait_recv()

        with scope("projside"):
            project(zz * 2 + 1 - x)

    def mix(zz):
        @pl.loop(0, 2)
        def _(i):
            block = zz * 2 + (x + i) % 2
            with scope("cwait"):

                @pl.when(block != s)
                def _():
                    c_arrival(block).wait_recv()

            with scope("local"):
                local(block)

    @pl.loop(0, nz)
    def _(zz):
        with scope("projown"):
            project(zz * 2 + x)

    @pl.loop(0, nz - 1)
    def _(k):
        project_side(level(k))

    @pl.loop(0, nz)
    def _(k):
        @pl.when(k == nz - 1)
        def _():
            project_side(level(k))

        mix(level(k))

    def drain():
        for k in range(1, n):
            c_copy((s + k) % n).wait_send()
        for j in range(3):
            for o in range(ny):
                w_copy(d, j, mate, w_near.at[o, j]).wait_send()
                if o:
                    w_copy(d, j, far(o), w_far.at[o, j]).wait_send()
        if bridged:

            @pl.when(inner)
            def _():
                for e in range(2):
                    c_pass(e).wait_send()

            @pl.when(is_end)
            def _():
                for sub in range(SUBS):
                    bridge(sub).wait_send()

        for sub in range(SUBS):
            h_copy(z, x, sub, side, h_side.at[0, sub, 0]).wait_send()
            for up in (True, False):
                for k in range(nz):

                    @pl.when(goes(k, up))
                    def _():
                        line(k, sub, up).wait_send()

                    if k:

                        @pl.when(crosses(k, up))
                        def _():
                            h_copy(z, x, sub, side, h_side.at[k, sub, int(up)]).wait_send()

    return drain


def project_block(h_all, w_all, p_all, rows, columns, scale, block):
    at = pl.ds(pl.multiple_of(block * rows, rows), rows)
    for j in range(3):
        value = dot(h_all[at, :], w_all[:, j * columns : (j + 1) * columns]).astype(BF16)
        if j == 1:
            value = (value.astype(F32) * scale).astype(BF16)
        p_all[at, j * columns : (j + 1) * columns] = value


def fill_tables(heads, rate, inner, inner_t, query_decay, key_decay):
    dim = query_decay.shape[2]
    row = lax.broadcasted_iota(jnp.int32, (BLOCK, BLOCK), 0).astype(F32)
    col = lax.broadcasted_iota(jnp.int32, (BLOCK, BLOCK), 1).astype(F32)
    place = lax.broadcasted_iota(jnp.int32, (BLOCK, dim), 0).astype(F32)
    spread = row - col
    for h in range(heads):
        g = rate[h]
        inner[h] = jnp.where(spread >= 0, jnp.exp(g * jnp.maximum(spread, 0.0)), 0.0)
        inner_t[h] = jnp.where(spread <= 0, jnp.exp(g * jnp.maximum(-spread, 0.0)), 0.0)
        query_decay[h] = jnp.exp(g * (place + 1.0))
        key_decay[h] = jnp.exp(g * (BLOCK - 1.0 - place))


def head_parts(columns, dim, h):
    return [slice(j * columns + h * dim, j * columns + (h + 1) * dim) for j in range(3)]


def local_block(heads, c_all, p_all, inner, inner_t, query_decay, key_decay, acc, s_term, r_term, block):
    columns = c_all.shape[1]
    dim = columns // heads
    at = pl.ds(pl.multiple_of(block * BLOCK, BLOCK), BLOCK)
    for h in range(heads):
        parts = head_parts(columns, dim, h)
        q, k, v = (p_all[at, part] for part in parts)
        c = c_all[at, parts[0]]
        mixed = (dot(c, v, NT) * inner[h]).astype(BF16)
        mixed_t = (dot(v, c, NT) * inner_t[h]).astype(BF16)
        scores_t = (dot(k, q, NT) * inner_t[h]).astype(BF16)
        s_term[block, h] = dot((k.astype(F32) * key_decay[h]).astype(BF16), v, TN)
        r_term[block, h] = dot((q.astype(F32) * query_decay[h]).astype(BF16), c, TN)
        acc[at, parts[0]] = dot(mixed, k)
        acc[at, parts[1]] = dot(mixed_t, q)
        acc[at, parts[2]] = dot(scores_t, c)


def chain_phase(heads, rate, c_all, p_all, g_all, query_decay, key_decay, acc, s_term, r_term, state, back):
    length, columns = c_all.shape
    dim = columns // heads
    blocks = length // BLOCK
    scale = dim ** (-0.5)
    state[...] = jnp.zeros_like(state)
    back[...] = jnp.zeros_like(back)

    @pl.loop(0, blocks)
    def _(i):
        for h in range(heads):
            block_decay = jnp.exp(jnp.full((1, dim), rate[h] * BLOCK, F32))
            parts = head_parts(columns, dim, h)

            at = pl.ds(pl.multiple_of(i * BLOCK, BLOCK), BLOCK)
            held = state[h]
            across = dot(c_all[at, parts[0]], held.astype(BF16), NT) * query_decay[h]
            g_all[at, parts[0]] = (acc[at, parts[0]] + across).astype(BF16)
            state[h] = held * block_decay + s_term[i, h]

            j = blocks - 1 - i
            at = pl.ds(pl.multiple_of(j * BLOCK, BLOCK), BLOCK)
            held = back[h]
            held_bf = held.astype(BF16)
            across = dot(p_all[at, parts[2]], held_bf, NT) * key_decay[h]
            g_all[at, parts[1]] = ((acc[at, parts[1]] + across) * scale).astype(BF16)
            across = dot(p_all[at, parts[1]], held_bf) * key_decay[h]
            g_all[at, parts[2]] = (acc[at, parts[2]] + across).astype(BF16)
            back[h] = held * block_decay + r_term[j, h]


def scatter_phase(
    n, m, h_all, w_all, g_all, dh, dq, dk, dv,
    part, ring, turned, near_out, near_in, far_out, far_in,
    r_send, r_recv, n_send, n_recv, f_send, f_recv,
):
    s = lax.axis_index("sp")
    d = lax.axis_index("dp")
    z, x = s // 2, s % 2
    y, core = d // 2, d % 2
    nz, ny = n // 2, m // 2
    rows, width = dh.shape
    depth, columns = dq.shape
    chunk = width // CHUNKS
    lanes = rows // 2
    mate = d + 1 - 2 * core
    me = x * (n - 1 - z) + (1 - x) * z

    def at_ring(p):
        p = (p + 2 * n) % n
        hi = p // nz
        return (hi * (n - 1 - p) + (1 - hi) * p) * 2 + hi

    def far(o):
        return ((y + o) % ny) * 2 + core

    right, left = at_ring(me + 1), at_ring(me - 1)

    def own(offset):
        return pl.multiple_of(at_ring(me + offset) * rows, rows)

    ready = set()

    def partial(q, *offsets):
        todo = [o % n for o in offsets if (q, o % n) not in ready]
        if not todo:
            return
        ready.update((q, o) for o in todo)
        bases = [own(o) for o in todo]
        with scope("partial", q, *todo):
            lhs = jnp.concatenate([g_all[pl.ds(base, rows), :] for base in bases], axis=0)
            value = dot(lhs, w_all[q * chunk : (q + 1) * chunk, :], NT).astype(BF16)
            for place, base in enumerate(bases):
                part[q, pl.ds(base, rows), :] = value[place * rows : (place + 1) * rows]

    def spot(way, piece):
        return way * (CHUNKS // 2) + piece // 2, (piece % 2) * lanes

    def r_copy(step, way, piece):
        q, lane = spot(way, piece)
        if step == 0:
            base = own(-1 if way == 0 else 1)
            src = part.at[q, pl.ds(pl.multiple_of(base + lane, lanes), lanes)]
        else:
            src = ring.at[step - 1, way, piece]
        return remote(
            src,
            ring.at[step, way, piece],
            r_send.at[step, way, piece],
            r_recv.at[step, way, piece],
            {"sp": right if way == 0 else left},
        )

    def process(step, piece):
        for way in range(2):
            offset = -(step + 2) if way == 0 else step + 2
            q, lane = spot(way, piece)
            partial(q, -(step + 2), step + 2)
            with scope("ring", step, way, piece):
                r_copy(step, way, piece).wait_recv()
            mine = part[q, pl.ds(pl.multiple_of(own(offset) + lane, lanes), lanes), :]
            total = (ring[step, way, piece].astype(F32) + mine.astype(F32)).astype(BF16)
            if step < n - 2:
                ring[step, way, piece] = total
                r_copy(step + 1, way, piece).start()
            else:
                dh[lane : lane + lanes, q * chunk : (q + 1) * chunk] = total

    def turn(slot, device):
        turned[slot] = h_all[:, pl.ds(pl.multiple_of(device * depth, depth), depth)].T

    def weight_part(slot, j):
        return dot(turned[slot], g_all[:, j * columns : (j + 1) * columns])

    def n_copy(o, j):
        return remote(
            near_out.at[o, j], near_in.at[o, j], n_send.at[o, j], n_recv.at[o, j], {"dp": mate}
        )

    def f_copy(o, j):
        return remote(
            far_out.at[o - 1, j], far_in.at[o - 1, j], f_send.at[o - 1, j], f_recv.at[o - 1, j], {"dp": far(o)}
        )

    def near(o, j):
        if j == 0:
            turn(0, far(o) + 1 - 2 * core)
        with scope("near", o, j):
            near_out[o, j] = weight_part(0, j).astype(BF16)
        n_copy(o, j).start()

    def chip_sum(o, j):
        if j == 0:
            turn(1, far(o))
        with scope("chip_sum", o, j):
            value = weight_part(1, j)
            n_copy(o, j).wait_recv()
            value = value + near_in[o, j].astype(F32)
        if o:
            far_out[o - 1, j] = value.astype(BF16)
            f_copy(o, j).start()
        else:
            (dq, dk, dv)[j][...] = value

    def weight(kind, o, j):
        return functools.partial(kind, o, j)

    tasks = []
    for o in list(range(1, ny)) + [0]:
        tasks += [weight(near, o, 0), weight(near, o, 1), weight(chip_sum, o, 0)]
        tasks += [weight(near, o, 2), weight(chip_sum, o, 1), weight(chip_sum, o, 2)]

    def work(count=1):
        for _ in range(count):
            if tasks:
                tasks.pop(0)()

    order = [q for k in range(CHUNKS // 2) for q in (k, CHUNKS // 2 + k)]
    for q in order:
        partial(q, -1, 1)
        way, first = divmod(q, CHUNKS // 2)
        for piece in (2 * first, 2 * first + 1):
            r_copy(0, way, piece).start()
    work()
    for q in order[:2]:
        partial(q, -2, 2)
    work(2)
    pairs = [(q, pair) for pair in [(-2, 2), (-3, 3), (n // 2, 0)] for q in order]
    for step in range(n - 1):
        for piece in range(PIECES):
            process(step, piece)
            while pairs and all((pairs[0][0], o % n) in ready for o in pairs[0][1]):
                pairs.pop(0)
            if pairs and (step < 2 or not tasks):
                q, pair = pairs.pop(0)
                partial(q, *pair)
                if step and piece % 2:
                    work()
            else:
                work()
    work(len(tasks))
    for j, out in enumerate((dq, dk, dv)):
        total = out[...]
        for o in range(1, ny):
            with scope("fwait", o, j):
                f_copy(o, j).wait_recv()
            total = total + far_in[o - 1, j].astype(F32)
        out[...] = total * (1.0 / m)
    for step in range(n - 1):
        for piece in range(PIECES):
            for way in range(2):
                r_copy(step, way, piece).wait_send()
    for o in range(ny):
        for j in range(3):
            n_copy(o, j).wait_send()
            if o:
                f_copy(o, j).wait_send()


def whole_kernel(n, m, heads, rate, h_in, c_in, wq, wk, wv, dh, dq, dk, dv, *scratch):
    h_all, c_all, w_all, p_all, g_all, state, back = scratch[:7]
    decays, (acc, s_term, r_term) = scratch[7:11], scratch[11:14]
    gather_refs, rest = scratch[14:28], scratch[28:]
    columns = wq.shape[1]
    project = functools.partial(
        project_block, h_all, w_all, p_all, h_in.shape[0], columns, (columns // heads) ** (-0.5)
    )
    local = functools.partial(local_block, heads, c_all, p_all, *decays, acc, s_term, r_term)
    tables = functools.partial(fill_tables, heads, rate, *decays)
    drain = gather_phase(
        n, m, project, local, tables, h_in, c_in, wq, wk, wv, h_all, c_all, w_all, *gather_refs
    )
    with scope("chain"):
        chain_phase(heads, rate, c_all, p_all, g_all, *decays[2:], acc, s_term, r_term, state, back)
    scatter_phase(n, m, h_all, w_all, g_all, dh, dq, dk, dv, *rest)
    with scope("drain"):
        drain()


def whole(n, m, rate, h, c, wq, wk, wv):
    rows, width = h.shape
    depth, columns = wq.shape
    heads = rate.shape[0]
    dim = columns // heads
    length = rows * n
    ny = m // 2
    vmem = pl.BlockSpec(memory_space=pltpu.VMEM)
    dma = pltpu.SemaphoreType.DMA
    return pl.pallas_call(
        functools.partial(whole_kernel, n, m, heads),
        out_shape=(pltpu.VMEM((rows, width), BF16),)
        + (pltpu.VMEM((depth, columns), F32),) * 3,
        in_specs=[pl.BlockSpec(memory_space=pltpu.SMEM)]
        + [pl.BlockSpec(memory_space=pl.ANY)] * 5,
        out_specs=(vmem,) * 4,
        scratch_shapes=[
            pltpu.VMEM((length, width), BF16),
            pltpu.VMEM((length, columns), BF16),
            pltpu.VMEM((depth * m, 3 * columns), BF16),
            pltpu.VMEM((length, 3 * columns), BF16),
            pltpu.VMEM((length, 3 * columns), BF16),
            pltpu.VMEM((heads, dim, dim), F32),
            pltpu.VMEM((heads, dim, dim), F32),
            pltpu.VMEM((heads, BLOCK, BLOCK), F32),
            pltpu.VMEM((heads, BLOCK, BLOCK), F32),
            pltpu.VMEM((heads, BLOCK, dim), F32),
            pltpu.VMEM((heads, BLOCK, dim), F32),
            pltpu.VMEM((length, 3 * columns), F32),
            pltpu.VMEM((length // BLOCK, heads, dim, dim), F32),
            pltpu.VMEM((length // BLOCK, heads, dim, dim), F32),
            pltpu.VMEM((rows, columns * n), BF16),
            pltpu.VMEM((2, rows, columns), BF16),
            dma((6,)),
            dma((n, SUBS)),
            dma((n // 2, SUBS, 2)),
            dma((n // 2, SUBS, 2)),
            dma((SUBS,)),
            dma((n,)),
            dma((n,)),
            dma((2,)),
            dma((2,)),
            dma((ny, 3)),
            dma((ny, 3)),
            dma((m, 3)),
            pltpu.VMEM((CHUNKS, length, width // CHUNKS), BF16),
            pltpu.VMEM((n - 1, 2, PIECES, rows // 2, width // CHUNKS), BF16),
            pltpu.VMEM((2, depth, length), BF16),
            pltpu.VMEM((ny, 3, depth, columns), BF16),
            pltpu.VMEM((ny, 3, depth, columns), BF16),
            pltpu.VMEM((ny - 1, 3, depth, columns), BF16),
            pltpu.VMEM((ny - 1, 3, depth, columns), BF16),
            dma((n - 1, 2, PIECES)),
            dma((n - 1, 2, PIECES)),
            dma((ny, 3)),
            dma((ny, 3)),
            dma((ny - 1, 3)),
            dma((ny - 1, 3)),
        ],
        compiler_params=pltpu.CompilerParams(
            collective_id=0, has_side_effects=True, vmem_limit_bytes=VMEM_LIMIT
        ),
        name="whole",
    )(rate, h, c, wq, wk, wv)


def finish_kernel(count, *refs):
    ins, outs, sems = refs[:count], refs[count : 2 * count], refs[2 * count]
    moves = [pltpu.make_async_copy(ins[i], outs[i], sems.at[i]) for i in range(count)]
    for move in moves:
        move.start()
    for move in moves:
        move.wait()


def finish(*arrays):
    count = len(arrays)
    return pl.pallas_call(
        functools.partial(finish_kernel, count),
        out_shape=tuple(jax.ShapeDtypeStruct(a.shape, a.dtype) for a in arrays),
        in_specs=[pl.BlockSpec(memory_space=pltpu.VMEM)] * count,
        out_specs=(pl.BlockSpec(memory_space=pl.ANY),) * count,
        scratch_shapes=[pltpu.SemaphoreType.DMA((count,))],
        compiler_params=pltpu.CompilerParams(vmem_limit_bytes=4 * 1024 * 1024),
        name="finish",
    )(*arrays)


def body(n, m, hidden_in, mix_cotangent, query_weight, key_weight, value_weight, decay_log):
    dh, dq, dk, dv = finish(
        *whole(
            n, m, decay_log, hidden_in[0], mix_cotangent[0], query_weight, key_weight, value_weight
        )
    )
    return dh[None], dq, dk, dv


def solution(mesh):
    placed = (
        P("dp", "sp", None),
        P("dp", "sp", None),
        P("dp", "sp"),
        P("dp", "sp"),
        P("dp", "sp"),
        P("sp"),
    )
    return jax.shard_map(
        functools.partial(body, mesh.shape["sp"], mesh.shape["dp"]),
        mesh=mesh,
        in_specs=placed,
        out_specs=(P("dp", "sp", None), P("dp", "sp"), P("dp", "sp"), P("dp", "sp")),
        check_vma=False,
    )
```

```python
import functools

import jax
import jax.numpy as jnp
from jax import lax
from jax.experimental import pallas as pl
from jax.experimental.pallas import tpu as pltpu
from jax.sharding import PartitionSpec as P

BLOCK = 128
SUBS = 2
CHUNKS = 4
PIECES = 4
F32 = jnp.float32
BF16 = jnp.bfloat16
MESH = pl.DeviceIdType.MESH
NT = (((1,), (1,)), ((), ()))
TN = (((0,), (0,)), ((), ()))
VMEM_LIMIT = 58 * 1024 * 1024


def dot(a, b, dims=(((1,), (0,)), ((), ()))):
    return lax.dot_general(a, b, dims, preferred_element_type=F32)


def scope(name, *tags):
    return jax.named_scope("#".join([name] + [str(t) for t in tags]))


def remote(src, dst, send, recv, where):
    return pltpu.make_async_remote_copy(
        src_ref=src, dst_ref=dst, send_sem=send, recv_sem=recv, device_id=where, device_id_type=MESH
    )


def greet(always, sometimes):
    barrier = pltpu.get_barrier_semaphore()
    count = len(always)
    for where in always:
        pl.semaphore_signal(barrier, inc=1, device_id=where, device_id_type=MESH)
    for there, where in sometimes:
        count = count + jnp.where(there, 1, 0)

        @pl.when(there)
        def _():
            pl.semaphore_signal(barrier, inc=1, device_id=where, device_id_type=MESH)

    return lambda: pl.semaphore_wait(barrier, count)


def gather_phase(
    n, m, project, local, tables, h_in, c_in, wq, wk, wv, h_all, c_all, w_all, c_own, c_via, l_sem,
    h_recv, h_line, h_side, h_bridge, c_send, c_recv, v_send, v_recv, w_far, w_near, w_recv,
):
    s = lax.axis_index("sp")
    d = lax.axis_index("dp")
    z, x = s // 2, s % 2
    y, core = d // 2, d % 2
    nz, ny = n // 2, m // 2
    rows = h_in.shape[0]
    sub_rows = rows // SUBS
    depth, columns = wq.shape
    side = s + 1 - 2 * x
    mate = d + 1 - 2 * core
    bridged = nz > 2
    is_end = jnp.logical_or(z == 0, z == nz - 1)
    inner = jnp.logical_not(is_end)
    inward = jnp.where(z == 0, s + 2, s - 2)

    def far(o):
        return ((y + o) % ny) * 2 + core

    arrived = greet(
        [{"sp": side}, {"dp": mate}] + [{"dp": far(o)} for o in range(1, ny)],
        [(z >= 1, {"sp": s - 2}), (z + 1 < nz, {"sp": s + 2})],
    )

    def part_rows(block):
        return pl.ds(pl.multiple_of(block * rows, rows), rows)

    def part_columns(block):
        return pl.ds(pl.multiple_of(block * columns, columns), columns)

    own_depth = pl.ds(pl.multiple_of(d * depth, depth), depth)
    loads = [pltpu.make_async_copy(h_in, h_all.at[part_rows(s)], l_sem.at[0])]
    for j, w in enumerate((wq, wk, wv)):
        place = w_all.at[own_depth, pl.ds(j * columns, columns)]
        loads.append(pltpu.make_async_copy(w, place, l_sem.at[1 + j]))
    loads.append(pltpu.make_async_copy(c_in, c_own, l_sem.at[4]))
    mine = c_in.at[:, part_columns(s)]
    loads.append(pltpu.make_async_copy(mine, c_all.at[part_rows(s)], l_sem.at[5]))
    for load in loads:
        load.start()

    def h_copy(src_z, src_x, sub, dest, send):
        block = src_z * 2 + src_x
        place = pl.ds(pl.multiple_of(block * rows + sub * sub_rows, sub_rows), sub_rows)
        return remote(h_all.at[place], h_all.at[place], send, h_recv.at[block, sub], {"sp": dest})

    def w_copy(src_d, j, dest, send):
        place = w_all.at[
            pl.ds(pl.multiple_of(src_d * depth, depth), depth), pl.ds(j * columns, columns)
        ]
        return remote(place, place, send, w_recv.at[src_d, j], {"dp": dest})

    def c_copy(to):
        return remote(
            c_own.at[:, part_columns(to)], c_all.at[part_rows(s)], c_send.at[to], c_recv.at[s], {"sp": to}
        )

    def c_arrival(block):
        return remote(
            c_all.at[part_rows(block)], c_all.at[part_rows(block)], c_send.at[block], c_recv.at[block], {"sp": side}
        )

    def end_block(e, column):
        return e * (nz - 1) * 2 + column

    def c_cross(e):
        to = end_block(e, 1 - x)
        return remote(
            c_own.at[:, part_columns(to)], c_via.at[e], c_send.at[to], v_recv.at[e], {"sp": side}
        )

    def c_pass(e):
        return remote(
            c_via.at[e], c_all.at[part_rows(side)], v_send.at[e], c_recv.at[side], {"sp": end_block(e, x)}
        )

    def line(k, sub, up):
        source = (z - k) if up else (z + k)
        dest = (s + 2) if up else (s - 2)
        return h_copy(source, x, sub, dest, h_line.at[k, sub, int(up)])

    def goes(k, up):
        if up:
            return jnp.logical_and(z - k >= 0, z + 1 < nz)
        return jnp.logical_and(z + k < nz, z >= 1)

    def arrives(k, up):
        return (z - k >= 0) if up else (z + k < nz)

    def crosses(k, up):
        here = arrives(k, up)
        if not bridged or k != 1:
            return here
        return jnp.logical_and(here, (z != 1) if up else (z != nz - 2))

    def bridge(sub):
        return h_copy(z, 1 - x, sub, inward, h_bridge.at[sub])

    with scope("greet"):
        loads[0].wait()
        arrived()
    for sub in range(SUBS):
        for up in (True, False):

            @pl.when(goes(0, up))
            def _():
                line(0, sub, up).start()

        h_copy(z, x, sub, side, h_side.at[0, sub, 0]).start()
    for j in range(3):
        loads[1 + j].wait()
        for o in range(1, ny):
            w_copy(d, j, far(o), w_far.at[o, j]).start()
        w_copy(d, j, mate, w_near.at[0, j]).start()
    loads[4].wait()
    loads[5].wait()
    if bridged:

        @pl.when(inner)
        def _():
            for e in range(2):
                c_cross(e).start()
            c_copy(side).start()

    tables()

    def pass_weights(j):
        for o in range(1, ny):
            with scope("wfar", j):
                w_copy(far(o), j, mate, w_near.at[o, j]).wait_recv()
            w_copy(far(o), j, mate, w_near.at[o, j]).start()

    def send_level(k):
        for up in (True, False):
            to_z = (z + k) if up else (z - k)

            @pl.when((to_z < nz) if up else (to_z >= 0))
            def _():
                c_copy(to_z * 2 + x).start()
                c_copy(to_z * 2 + 1 - x).start()

    def send_column(k):
        for up in (True, False):
            to_z = (z + k) if up else (z - k)

            @pl.when((to_z < nz) if up else (to_z >= 0))
            def _():
                c_copy(to_z * 2 + x).start()

            @pl.when(to_z == (nz - 1 if up else 0))
            def _():
                c_cross(int(up)).wait_recv()
                c_pass(int(up)).start()

    def send_across(k):
        for up in (True, False):
            to_z = (z + k) if up else (z - k)

            @pl.when((to_z < nz - 1) if up else (to_z >= 1))
            def _():
                c_copy(to_z * 2 + 1 - x).start()

    upper = z // ((nz + 1) // 2)
    from_low = upper * (nz - 1) + (1 - 2 * upper) * z

    def level(k):
        low = jnp.where(k == 0, from_low, jnp.where(k - 1 < from_low, k - 1, k))
        return upper * (nz - 1) + (1 - 2 * upper) * low

    def side_wait(zz):
        fresh = jnp.logical_not(jnp.logical_and(is_end, zz == z)) if bridged else True
        with scope("sidewait"):

            @pl.when(fresh)
            def _():
                for sub in range(SUBS):
                    h_copy(zz, 1 - x, sub, side, h_side.at[0, sub, 0]).wait_recv()

    def wait_weights(j):
        w_copy(mate, j, mate, w_near.at[0, j]).wait_recv()
        for o in range(1, ny):
            other = far(o) + 1 - 2 * core
            with scope("wmate", j):
                w_copy(other, j, mate, w_near.at[o, j]).wait_recv()

    def early():
        for j in range(2):
            wait_weights(j)
        with scope("early"):

            @pl.loop(0, nz - 1)
            def _(k):
                project(level(k) * 2 + x, (0, 1))

            side_wait(level(0))
            project(level(0) * 2 + 1 - x, (0, 1))

    passed = 0
    for k in range(1, nz):
        if bridged and k == nz - 1:

            @pl.when(inner)
            def _():
                send_column(1)

        for sub in range(SUBS):
            for up in (True, False):

                @pl.when(arrives(k, up))
                def _():
                    source = (z - k) if up else (z + k)
                    with scope("hline", k, sub, up):
                        h_copy(source, x, sub, side, h_side.at[k, sub, int(up)]).wait_recv()

                @pl.when(crosses(k, up))
                def _():
                    source = (z - k) if up else (z + k)
                    h_copy(source, x, sub, side, h_side.at[k, sub, int(up)]).start()

                @pl.when(goes(k, up))
                def _():
                    line(k, sub, up).start()

            if bridged and k == 1:

                @pl.when(is_end)
                def _():
                    h_copy(z, 1 - x, sub, side, h_side.at[0, sub, 0]).wait_recv()
                    bridge(sub).start()

            if bridged and (k, sub) in ((nz - 2, 0), (nz - 2, SUBS - 1), (nz - 1, 0)):
                if passed == 2:

                    @pl.when(is_end)
                    def _():
                        for past in range(2, nz - 1):
                            send_level(past)

                    early()
                pass_weights(passed)
                passed += 1
        if bridged and k == 1:

            @pl.when(is_end)
            def _():
                c_copy(side).start()
                send_level(1)

    if bridged:

        @pl.when(inner)
        def _():
            send_across(1)

    else:
        c_copy(side).start()
        for k in range(1, nz):
            send_level(k)

    for j in range(passed, 3):
        if j == 2:
            early()
        pass_weights(j)
    wait_weights(2)
    if bridged:

        @pl.when(inner)
        def _():
            for k in range(2, nz):
                send_column(k)
                send_across(k)

    @pl.loop(0, nz - 1)
    def _(k):
        project(level(k) * 2 + x, (2,))

    project(level(0) * 2 + 1 - x, (2,))
    project(level(nz - 1) * 2 + x, (0, 1, 2))

    @pl.loop(0, 2 * nz - 1)
    def _(t):
        last = 2 * nz - 4
        held = jnp.logical_and(t != last, jnp.logical_or(t == 0, t >= nz - 1))
        mixes = jnp.where(is_end, held, t % 2 == 0)
        late = jnp.where(t < nz - 1, t, jnp.where(t < last, t - nz + 2, t - nz + 1))
        late = jnp.where(t == last, nz - 1, late)
        zz = level(jnp.where(is_end, late, (t + 1) // 2))
        if bridged:

            @pl.when(jnp.logical_and(is_end, t == 1))
            def _():
                send_level(nz - 1)

        @pl.when(jnp.logical_not(mixes))
        def _():
            side_wait(zz)
            with scope("projside"):
                project(zz * 2 + 1 - x, (0, 1, 2))

        @pl.when(mixes)
        def _():
            with scope("cwait"):
                for column in range(2):

                    @pl.when(zz * 2 + column != s)
                    def _():
                        c_arrival(zz * 2 + column).wait_recv()

            with scope("local"):
                local(zz * 2, zz * 2 + 1)

    def drain():
        for k in range(1, n):
            c_copy((s + k) % n).wait_send()
        for j in range(3):
            for o in range(ny):
                w_copy(d, j, mate, w_near.at[o, j]).wait_send()
                if o:
                    w_copy(d, j, far(o), w_far.at[o, j]).wait_send()
        if bridged:

            @pl.when(inner)
            def _():
                for e in range(2):
                    c_pass(e).wait_send()

            @pl.when(is_end)
            def _():
                for sub in range(SUBS):
                    bridge(sub).wait_send()

        for sub in range(SUBS):
            h_copy(z, x, sub, side, h_side.at[0, sub, 0]).wait_send()
            for up in (True, False):
                for k in range(nz):

                    @pl.when(goes(k, up))
                    def _():
                        line(k, sub, up).wait_send()

                    if k:

                        @pl.when(crosses(k, up))
                        def _():
                            h_copy(z, x, sub, side, h_side.at[k, sub, int(up)]).wait_send()

    return drain


def project_block(h_all, w_all, p_all, rows, columns, scale, block, which):
    at = pl.ds(pl.multiple_of(block * rows, rows), rows)
    for j in which:
        value = dot(h_all[at, :], w_all[:, j * columns : (j + 1) * columns]).astype(BF16)
        if j == 1:
            value = (value.astype(F32) * scale).astype(BF16)
        p_all[at, j * columns : (j + 1) * columns] = value


def fill_tables(heads, rate, inner, inner_t, query_decay, key_decay):
    dim = query_decay.shape[2]
    row = lax.broadcasted_iota(jnp.int32, (BLOCK, BLOCK), 0).astype(F32)
    col = lax.broadcasted_iota(jnp.int32, (BLOCK, BLOCK), 1).astype(F32)
    place = lax.broadcasted_iota(jnp.int32, (BLOCK, dim), 0).astype(F32)
    spread = row - col
    for h in range(heads):
        g = rate[h]
        inner[h] = jnp.where(spread >= 0, jnp.exp(g * jnp.maximum(spread, 0.0)), 0.0)
        inner_t[h] = jnp.where(spread <= 0, jnp.exp(g * jnp.maximum(-spread, 0.0)), 0.0)
        query_decay[h] = jnp.exp(g * (place + 1.0))
        key_decay[h] = jnp.exp(g * (BLOCK - 1.0 - place))


def head_parts(columns, dim, h):
    return [slice(j * columns + h * dim, j * columns + (h + 1) * dim) for j in range(3)]


def local_block(heads, c_all, p_all, inner, inner_t, query_decay, key_decay, acc, s_term, r_term, *blocks):
    columns = c_all.shape[1]
    dim = columns // heads
    for h, block in ((h, block) for h in range(heads) for block in blocks):
        at = pl.ds(pl.multiple_of(block * BLOCK, BLOCK), BLOCK)
        parts = head_parts(columns, dim, h)
        q, k, v = (p_all[at, part] for part in parts)
        c = c_all[at, parts[0]]
        mixed = (dot(c, v, NT) * inner[h]).astype(BF16)
        mixed_t = (dot(v, c, NT) * inner_t[h]).astype(BF16)
        scores_t = (dot(k, q, NT) * inner_t[h]).astype(BF16)
        s_term[block, h] = dot((k.astype(F32) * key_decay[h]).astype(BF16), v, TN)
        r_term[block, h] = dot((q.astype(F32) * query_decay[h]).astype(BF16), c, TN)
        acc[at, parts[0]] = dot(mixed, k)
        acc[at, parts[1]] = dot(mixed_t, q)
        acc[at, parts[2]] = dot(scores_t, c)


def chain_phase(heads, rate, c_all, p_all, g_all, query_decay, key_decay, acc, s_term, r_term, state, back):
    length, columns = c_all.shape
    dim = columns // heads
    blocks = length // BLOCK
    scale = dim ** (-0.5)
    state[...] = jnp.zeros_like(state)
    back[...] = jnp.zeros_like(back)

    for i in range(blocks):
        for h in range(heads):
            block_decay = jnp.exp(jnp.full((1, dim), rate[h] * BLOCK, F32))
            parts = head_parts(columns, dim, h)

            at = slice(i * BLOCK, (i + 1) * BLOCK)
            held = state[h]
            across = dot(c_all[at, parts[0]], held.astype(BF16), NT) * query_decay[h]
            g_all[at, parts[0]] = (acc[at, parts[0]] + across).astype(BF16)
            state[h] = held * block_decay + s_term[i, h]

            j = blocks - 1 - i
            at = slice(j * BLOCK, (j + 1) * BLOCK)
            held = back[h]
            held_bf = held.astype(BF16)
            across = dot(p_all[at, parts[2]], held_bf, NT) * key_decay[h]
            g_all[at, parts[1]] = ((acc[at, parts[1]] + across) * scale).astype(BF16)
            across = dot(p_all[at, parts[1]], held_bf) * key_decay[h]
            g_all[at, parts[2]] = (acc[at, parts[2]] + across).astype(BF16)
            back[h] = held * block_decay + r_term[j, h]


def scatter_phase(
    n, m, drain, h_all, w_all, g_all, dh, dq, dk, dv,
    part, ring, turned, near_out, near_in, far_out, far_in,
    r_send, r_recv, n_send, n_recv, f_send, f_recv,
):
    s = lax.axis_index("sp")
    d = lax.axis_index("dp")
    z, x = s // 2, s % 2
    y, core = d // 2, d % 2
    nz, ny = n // 2, m // 2
    rows, width = dh.shape
    depth, columns = dq.shape
    chunk = width // CHUNKS
    lanes = rows // 2
    mate = d + 1 - 2 * core
    me = x * (n - 1 - z) + (1 - x) * z

    def at_ring(p):
        p = (p + 2 * n) % n
        hi = p // nz
        return (hi * (n - 1 - p) + (1 - hi) * p) * 2 + hi

    def far(o):
        return ((y + o) % ny) * 2 + core

    right, left = at_ring(me + 1), at_ring(me - 1)

    def own(offset):
        return pl.multiple_of(at_ring(me + offset) * rows, rows)

    ready = set()

    def partial(q, *offsets):
        todo = [o % n for o in offsets if (q, o % n) not in ready]
        if not todo:
            return
        ready.update((q, o) for o in todo)
        bases = [own(o) for o in todo]
        with scope("partial", q, *todo):
            lhs = jnp.concatenate([g_all[pl.ds(base, rows), :] for base in bases], axis=0)
            value = dot(lhs, w_all[q * chunk : (q + 1) * chunk, :], NT).astype(BF16)
            for place, base in enumerate(bases):
                part[q, pl.ds(base, rows), :] = value[place * rows : (place + 1) * rows]

    def spot(way, piece):
        return way * (CHUNKS // 2) + piece // 2, (piece % 2) * lanes

    def r_copy(step, way, piece):
        q, lane = spot(way, piece)
        if step == 0:
            base = own(-1 if way == 0 else 1)
            src = part.at[q, pl.ds(pl.multiple_of(base + lane, lanes), lanes)]
        else:
            src = ring.at[step - 1, way, piece]
        return remote(
            src,
            ring.at[step, way, piece],
            r_send.at[step],
            r_recv.at[step, way, piece],
            {"sp": right if way == 0 else left},
        )

    def process(step, piece):
        for way in range(2):
            offset = -(step + 2) if way == 0 else step + 2
            q, lane = spot(way, piece)
            partial(q, -(step + 2), step + 2)
            with scope("ring", step, way, piece):
                r_copy(step, way, piece).wait_recv()
            mine = part[q, pl.ds(pl.multiple_of(own(offset) + lane, lanes), lanes), :]
            total = (ring[step, way, piece].astype(F32) + mine.astype(F32)).astype(BF16)
            if step < n - 2:
                ring[step, way, piece] = total
                r_copy(step + 1, way, piece).start()
            else:
                dh[lane : lane + lanes, q * chunk : (q + 1) * chunk] = total

    def turn(slot, device):
        turned[slot] = h_all[:, pl.ds(pl.multiple_of(device * depth, depth), depth)].T

    def weight_part(slot, j):
        return dot(turned[slot], g_all[:, j * columns : (j + 1) * columns])

    def n_copy(o, j):
        return remote(
            near_out.at[o, j], near_in.at[o, j], n_send.at[o, j], n_recv.at[o, j], {"dp": mate}
        )

    def f_copy(o, j):
        return remote(
            far_out.at[o - 1, j], far_in.at[o - 1, j], f_send.at[o - 1, j], f_recv.at[o - 1, j], {"dp": far(o)}
        )

    def near(o, j):
        if j == 0:
            turn(0, far(o) + 1 - 2 * core)
        with scope("near", o, j):
            near_out[o, j] = weight_part(0, j).astype(BF16)
        n_copy(o, j).start()

    def chip_sum(o, j):
        if j == 0:
            turn(1, far(o))
        with scope("chip_sum", o, j):
            value = weight_part(1, j)
            n_copy(o, j).wait_recv()
            value = value + near_in[o, j].astype(F32)
        if o:
            far_out[o - 1, j] = value.astype(BF16)
            f_copy(o, j).start()
        else:
            (dq, dk, dv)[j][...] = value

    def weight(kind, o, j):
        return functools.partial(kind, o, j)

    tasks = []
    for o in list(range(1, ny)) + [0]:
        first = [weight(near, o, 0), weight(chip_sum, o, 0)]
        later = [weight(near, o, 1), weight(near, o, 2), weight(chip_sum, o, 1), weight(chip_sum, o, 2)]
        tasks += first + later if o else [first[0], *later[:2], first[1], *later[2:]]

    def work(count=1):
        for _ in range(count):
            if tasks:
                tasks.pop(0)()

    order = [q for k in range(CHUNKS // 2) for q in (k, CHUNKS // 2 + k)]
    for spot_in_order, q in enumerate(order):
        if spot_in_order == 2:
            work()
        partial(q, -1, 1)
        way, first = divmod(q, CHUNKS // 2)
        for piece in (2 * first, 2 * first + 1):
            r_copy(0, way, piece).start()
    partial(order[0], -2, 2)
    work()
    partial(order[1], -2, 2)
    work()
    pairs = [(q, pair) for pair in [(-2, 2), (-3, 3), (n // 2, 0)] for q in order]
    def finish_weight(j):
        out = (dq, dk, dv)[j]
        total = out[...]
        for o in range(1, ny):
            with scope("fwait", o, j):
                f_copy(o, j).wait_recv()
            total = total + far_in[o - 1, j].astype(F32)
        out[...] = total * (1.0 / m)
        for o in range(1, ny):
            f_copy(o, j).wait_send()

    def sent(step):
        pltpu.make_async_copy(ring.at[step], ring.at[step], r_send.at[step]).wait()

    def settle():
        for o in range(ny):
            for j in range(3):
                n_copy(o, j).wait_send()
        drain()

    for step in range(n - 1):
        for piece in range(PIECES):
            if step == n - 2 and piece != 2:
                finish_weight(min(piece, 2))
            if step > 1 and piece == 0:
                sent(step - 2)
            if step == n - 3 and piece == 0:
                work(len(tasks))
                settle()
            process(step, piece)
            while pairs and all((pairs[0][0], o % n) in ready for o in pairs[0][1]):
                pairs.pop(0)
            if pairs and (step < 2 or not tasks):
                q, pair = pairs.pop(0)
                partial(q, *pair)
                if step and piece % 2:
                    work()
            else:
                work()
    with scope("tail"):
        sent(n - 3)
        sent(n - 2)


def whole_kernel(n, m, heads, rate, h_in, c_in, wq, wk, wv, dh, dq, dk, dv, *scratch):
    h_all, c_all, w_all, p_all, g_all, state, back = scratch[:7]
    decays, (acc, s_term, r_term) = scratch[7:11], scratch[11:14]
    gather_refs, rest = scratch[14:28], scratch[28:]
    columns = wq.shape[1]
    project = functools.partial(
        project_block, h_all, w_all, p_all, h_in.shape[0], columns, (columns // heads) ** (-0.5)
    )
    local = functools.partial(local_block, heads, c_all, p_all, *decays, acc, s_term, r_term)
    tables = functools.partial(fill_tables, heads, rate, *decays)
    drain = gather_phase(
        n, m, project, local, tables, h_in, c_in, wq, wk, wv, h_all, c_all, w_all, *gather_refs
    )
    with scope("chain"):
        chain_phase(heads, rate, c_all, p_all, g_all, *decays[2:], acc, s_term, r_term, state, back)
    scatter_phase(n, m, drain, h_all, w_all, g_all, dh, dq, dk, dv, *rest)


def whole(n, m, rate, h, c, wq, wk, wv):
    rows, width = h.shape
    depth, columns = wq.shape
    heads = rate.shape[0]
    dim = columns // heads
    length = rows * n
    ny = m // 2
    vmem = pl.BlockSpec(memory_space=pltpu.VMEM)
    dma = pltpu.SemaphoreType.DMA
    return pl.pallas_call(
        functools.partial(whole_kernel, n, m, heads),
        out_shape=(pltpu.VMEM((rows, width), BF16),)
        + (pltpu.VMEM((depth, columns), F32),) * 3,
        in_specs=[pl.BlockSpec(memory_space=pltpu.SMEM)]
        + [pl.BlockSpec(memory_space=pl.ANY)] * 5,
        out_specs=(vmem,) * 4,
        scratch_shapes=[
            pltpu.VMEM((length, width), BF16),
            pltpu.VMEM((length, columns), BF16),
            pltpu.VMEM((depth * m, 3 * columns), BF16),
            pltpu.VMEM((length, 3 * columns), BF16),
            pltpu.VMEM((length, 3 * columns), BF16),
            pltpu.VMEM((heads, dim, dim), F32),
            pltpu.VMEM((heads, dim, dim), F32),
            pltpu.VMEM((heads, BLOCK, BLOCK), F32),
            pltpu.VMEM((heads, BLOCK, BLOCK), F32),
            pltpu.VMEM((heads, BLOCK, dim), F32),
            pltpu.VMEM((heads, BLOCK, dim), F32),
            pltpu.VMEM((length, 3 * columns), F32),
            pltpu.VMEM((length // BLOCK, heads, dim, dim), F32),
            pltpu.VMEM((length // BLOCK, heads, dim, dim), F32),
            pltpu.VMEM((rows, columns * n), BF16),
            pltpu.VMEM((2, rows, columns), BF16),
            dma((6,)),
            dma((n, SUBS)),
            dma((n // 2, SUBS, 2)),
            dma((n // 2, SUBS, 2)),
            dma((SUBS,)),
            dma((n,)),
            dma((n,)),
            dma((2,)),
            dma((2,)),
            dma((ny, 3)),
            dma((ny, 3)),
            dma((m, 3)),
            pltpu.VMEM((CHUNKS, length, width // CHUNKS), BF16),
            pltpu.VMEM((n - 1, 2, PIECES, rows // 2, width // CHUNKS), BF16),
            pltpu.VMEM((2, depth, length), BF16),
            pltpu.VMEM((ny, 3, depth, columns), BF16),
            pltpu.VMEM((ny, 3, depth, columns), BF16),
            pltpu.VMEM((ny - 1, 3, depth, columns), BF16),
            pltpu.VMEM((ny - 1, 3, depth, columns), BF16),
            dma((n - 1,)),
            dma((n - 1, 2, PIECES)),
            dma((ny, 3)),
            dma((ny, 3)),
            dma((ny - 1, 3)),
            dma((ny - 1, 3)),
        ],
        compiler_params=pltpu.CompilerParams(
            collective_id=0, has_side_effects=True, vmem_limit_bytes=VMEM_LIMIT
        ),
        name="whole",
    )(rate, h, c, wq, wk, wv)


def finish_kernel(count, *refs):
    ins, outs, sems = refs[:count], refs[count : 2 * count], refs[2 * count]
    moves = [pltpu.make_async_copy(ins[i], outs[i], sems.at[i]) for i in range(count)]
    for move in moves:
        move.start()
    for move in moves:
        move.wait()


def finish(*arrays):
    count = len(arrays)
    return pl.pallas_call(
        functools.partial(finish_kernel, count),
        out_shape=tuple(jax.ShapeDtypeStruct(a.shape, a.dtype) for a in arrays),
        in_specs=[pl.BlockSpec(memory_space=pltpu.VMEM)] * count,
        out_specs=(pl.BlockSpec(memory_space=pl.ANY),) * count,
        scratch_shapes=[pltpu.SemaphoreType.DMA((count,))],
        compiler_params=pltpu.CompilerParams(vmem_limit_bytes=4 * 1024 * 1024),
        name="finish",
    )(*arrays)


def body(n, m, hidden_in, mix_cotangent, query_weight, key_weight, value_weight, decay_log):
    dh, dq, dk, dv = finish(
        *whole(
            n, m, decay_log, hidden_in[0], mix_cotangent[0], query_weight, key_weight, value_weight
        )
    )
    return dh[None], dq, dk, dv


def solution(mesh):
    placed = (
        P("dp", "sp", None),
        P("dp", "sp", None),
        P("dp", "sp"),
        P("dp", "sp"),
        P("dp", "sp"),
        P("sp"),
    )
    return jax.shard_map(
        functools.partial(body, mesh.shape["sp"], mesh.shape["dp"]),
        mesh=mesh,
        in_specs=placed,
        out_specs=(P("dp", "sp", None), P("dp", "sp"), P("dp", "sp"), P("dp", "sp")),
        check_vma=False,
    )
```

```python
import functools

import jax
import jax.numpy as jnp
from jax import lax
from jax.experimental import pallas as pl
from jax.experimental.pallas import tpu as pltpu
from jax.sharding import PartitionSpec as P

BLOCK = 128
SUBS = 2
CHUNKS = 4
PIECES = 4
F32 = jnp.float32
BF16 = jnp.bfloat16
MESH = pl.DeviceIdType.MESH
NT = (((1,), (1,)), ((), ()))
TN = (((0,), (0,)), ((), ()))
VMEM_LIMIT = 58 * 1024 * 1024


def dot(a, b, dims=(((1,), (0,)), ((), ()))):
    return lax.dot_general(a, b, dims, preferred_element_type=F32)


def scope(name, *tags):
    return jax.named_scope("#".join([name] + [str(t) for t in tags]))


def remote(src, dst, send, recv, where):
    return pltpu.make_async_remote_copy(
        src_ref=src, dst_ref=dst, send_sem=send, recv_sem=recv, device_id=where, device_id_type=MESH
    )


def greet(always, sometimes):
    barrier = pltpu.get_barrier_semaphore()
    count = len(always)
    for where in always:
        pl.semaphore_signal(barrier, inc=1, device_id=where, device_id_type=MESH)
    for there, where in sometimes:
        count = count + jnp.where(there, 1, 0)

        @pl.when(there)
        def _():
            pl.semaphore_signal(barrier, inc=1, device_id=where, device_id_type=MESH)

    return lambda: pl.semaphore_wait(barrier, count)


def gather_phase(
    n, m, project, local, tables, rate_in, rate, h_in, c_in, wq, wk, wv, h_all, c_all, w_all,
    c_own, c_via, l_sem,
    h_recv, h_sent, c_sent, c_recv, v_sent, v_recv, w_sent, w_near, w_recv,
):
    s = lax.axis_index("sp")
    d = lax.axis_index("dp")
    z, x = s // 2, s % 2
    y, core = d // 2, d % 2
    nz, ny = n // 2, m // 2
    rows = h_in.shape[0]
    sub_rows = rows // SUBS
    depth, columns = wq.shape
    side = s + 1 - 2 * x
    mate = d + 1 - 2 * core
    bridged = nz > 2
    is_end = jnp.logical_or(z == 0, z == nz - 1)
    inner = jnp.logical_not(is_end)
    inward = jnp.where(z == 0, s + 2, s - 2)

    def far(o):
        return ((y + o) % ny) * 2 + core

    def part_rows(block):
        return pl.ds(pl.multiple_of(block * rows, rows), rows)

    def part_columns(block):
        return pl.ds(pl.multiple_of(block * columns, columns), columns)

    own_depth = pl.ds(pl.multiple_of(d * depth, depth), depth)
    loads = [pltpu.make_async_copy(h_in, h_all.at[part_rows(s)], l_sem.at[0])]
    loads[0].start()
    arrived = greet(
        [{"sp": side}, {"dp": mate}] + [{"dp": far(o)} for o in range(1, ny)],
        [(z >= 1, {"sp": s - 2}), (z + 1 < nz, {"sp": s + 2})],
    )
    for j, w in enumerate((wq, wk, wv)):
        place = w_all.at[own_depth, pl.ds(j * columns, columns)]
        loads.append(pltpu.make_async_copy(w, place, l_sem.at[1 + j]))
    loads.append(pltpu.make_async_copy(c_in, c_own, l_sem.at[4]))
    mine = c_in.at[:, part_columns(s)]
    loads.append(pltpu.make_async_copy(mine, c_all.at[part_rows(s)], l_sem.at[5]))
    loads.append(pltpu.make_async_copy(rate_in, rate, l_sem.at[6]))
    for load in loads[1:]:
        load.start()

    def h_copy(src_z, src_x, sub, dest, send):
        block = src_z * 2 + src_x
        place = pl.ds(pl.multiple_of(block * rows + sub * sub_rows, sub_rows), sub_rows)
        return remote(h_all.at[place], h_all.at[place], send, h_recv.at[block, sub], {"sp": dest})

    def w_copy(src_d, j, dest, send, recv):
        place = w_all.at[
            pl.ds(pl.multiple_of(src_d * depth, depth), depth), pl.ds(j * columns, columns)
        ]
        return remote(place, place, send, recv, {"dp": dest})

    def w_far_copy(src_d, j, dest):
        return w_copy(src_d, j, dest, w_sent.at[0], w_recv.at[src_d // 2, j])

    def w_near_copy(src_d, j):
        return w_copy(src_d, j, mate, w_sent.at[1], w_near.at[j])

    def wait_bytes(ref, sem):
        pltpu.make_async_copy(ref, ref, sem).wait()

    def c_copy(to):
        return remote(
            c_own.at[:, part_columns(to)], c_all.at[part_rows(s)], c_sent, c_recv.at[s], {"sp": to}
        )

    def c_arrival(block):
        return remote(
            c_all.at[part_rows(block)], c_all.at[part_rows(block)], c_sent, c_recv.at[block], {"sp": side}
        )

    def end_block(e, column):
        return e * (nz - 1) * 2 + column

    def c_cross(e):
        to = end_block(e, 1 - x)
        return remote(
            c_own.at[:, part_columns(to)], c_via.at[e], c_sent, v_recv.at[e], {"sp": side}
        )

    def c_pass(e):
        return remote(
            c_via.at[e], c_all.at[part_rows(side)], v_sent, c_recv.at[side], {"sp": end_block(e, x)}
        )

    def line(k, sub, up):
        source = (z - k) if up else (z + k)
        dest = (s + 2) if up else (s - 2)
        return h_copy(source, x, sub, dest, h_sent.at[0])

    def goes(k, up):
        if up:
            return jnp.logical_and(z - k >= 0, z + 1 < nz)
        return jnp.logical_and(z + k < nz, z >= 1)

    def arrives(k, up):
        return (z - k >= 0) if up else (z + k < nz)

    def crosses(k, up):
        here = arrives(k, up)
        if not bridged or k != 1:
            return here
        return jnp.logical_and(here, (z != 1) if up else (z != nz - 2))

    def bridge(sub):
        return h_copy(z, 1 - x, sub, inward, h_sent.at[1])

    with scope("greet"):
        loads[0].wait()
        arrived()
    for sub in range(SUBS):
        for up in (True, False):

            @pl.when(goes(0, up))
            def _():
                line(0, sub, up).start()

        h_copy(z, x, sub, side, h_sent.at[1]).start()
    for j in range(3):
        loads[1 + j].wait()
        for o in range(1, ny):
            w_far_copy(d, j, far(o)).start()
        w_near_copy(d, j).start()
    loads[4].wait()
    loads[5].wait()
    if bridged:

        @pl.when(inner)
        def _():
            for e in range(2):
                c_cross(e).start()
            c_copy(side).start()

    loads[6].wait()
    tables()

    def pass_weights(j):
        for o in range(1, ny):
            with scope("wfar", j):
                w_far_copy(far(o), j, mate).wait_recv()
            w_near_copy(far(o), j).start()

    def send_level(k):
        for up in (True, False):
            to_z = (z + k) if up else (z - k)

            @pl.when((to_z < nz) if up else (to_z >= 0))
            def _():
                c_copy(to_z * 2 + x).start()
                c_copy(to_z * 2 + 1 - x).start()

    def send_column(k):
        for up in (True, False):
            to_z = (z + k) if up else (z - k)

            @pl.when((to_z < nz) if up else (to_z >= 0))
            def _():
                c_copy(to_z * 2 + x).start()

            @pl.when(to_z == (nz - 1 if up else 0))
            def _():
                c_cross(int(up)).wait_recv()
                c_pass(int(up)).start()

    def send_across(k):
        for up in (True, False):
            to_z = (z + k) if up else (z - k)

            @pl.when((to_z < nz - 1) if up else (to_z >= 1))
            def _():
                c_copy(to_z * 2 + 1 - x).start()

    upper = z // ((nz + 1) // 2)
    from_low = upper * (nz - 1) + (1 - 2 * upper) * z

    def level(k):
        low = jnp.where(k == 0, from_low, jnp.where(k - 1 < from_low, k - 1, k))
        return upper * (nz - 1) + (1 - 2 * upper) * low

    def side_wait(zz):
        fresh = jnp.logical_not(jnp.logical_and(is_end, zz == z)) if bridged else True
        with scope("sidewait"):

            @pl.when(fresh)
            def _():
                for sub in range(SUBS):
                    h_copy(zz, 1 - x, sub, side, h_sent.at[1]).wait_recv()

    def wait_weights(j):
        with scope("wmate", j):
            wait_bytes(w_all.at[pl.ds(0, ny * depth), pl.ds(j * columns, columns)], w_near.at[j])

    def early():
        for j in range(2):
            wait_weights(j)
        with scope("early"):

            @pl.loop(0, nz - 1)
            def _(k):
                project(level(k) * 2 + x, (0, 1))

            side_wait(level(0))
            project(level(0) * 2 + 1 - x, (0, 1))

    passed = 0
    for k in range(1, nz):
        if bridged and k == nz - 1:

            @pl.when(inner)
            def _():
                send_column(1)

        for sub in range(SUBS):
            for up in (True, False):

                @pl.when(arrives(k, up))
                def _():
                    source = (z - k) if up else (z + k)
                    with scope("hline", k, sub, up):
                        h_copy(source, x, sub, side, h_sent.at[1]).wait_recv()

                @pl.when(crosses(k, up))
                def _():
                    source = (z - k) if up else (z + k)
                    h_copy(source, x, sub, side, h_sent.at[1]).start()

                @pl.when(goes(k, up))
                def _():
                    line(k, sub, up).start()

            if bridged and k == 1:

                @pl.when(is_end)
                def _():
                    h_copy(z, 1 - x, sub, side, h_sent.at[1]).wait_recv()
                    bridge(sub).start()

            if bridged and (k, sub) in ((nz - 2, 0), (nz - 2, SUBS - 1), (nz - 1, 0)):
                if passed == 2:

                    @pl.when(is_end)
                    def _():
                        for past in range(2, nz - 1):
                            send_level(past)

                    early()
                pass_weights(passed)
                passed += 1
        if bridged and k == 1:

            @pl.when(is_end)
            def _():
                c_copy(side).start()
                send_level(1)

    if bridged:

        @pl.when(inner)
        def _():
            send_across(1)

    else:
        c_copy(side).start()
        for k in range(1, nz):
            send_level(k)

    for j in range(passed, 3):
        if j == 2:
            early()
        pass_weights(j)
    wait_weights(2)
    if bridged:

        @pl.when(inner)
        def _():
            for k in range(2, nz):
                send_column(k)
                send_across(k)

    @pl.loop(0, nz - 1)
    def _(k):
        project(level(k) * 2 + x, (2,))

    project(level(0) * 2 + 1 - x, (2,))
    project(level(nz - 1) * 2 + x, (0, 1, 2))

    @pl.loop(0, 2 * nz - 1)
    def _(t):
        last = 2 * nz - 4
        held = jnp.logical_and(t != last, jnp.logical_or(t == 0, t >= nz - 1))
        mixes = jnp.where(is_end, held, t % 2 == 0)
        late = jnp.where(t < nz - 1, t, jnp.where(t < last, t - nz + 2, t - nz + 1))
        late = jnp.where(t == last, nz - 1, late)
        zz = level(jnp.where(is_end, late, (t + 1) // 2))
        if bridged:

            @pl.when(jnp.logical_and(is_end, t == 1))
            def _():
                send_level(nz - 1)

        @pl.when(jnp.logical_not(mixes))
        def _():
            side_wait(zz)
            with scope("projside"):
                project(zz * 2 + 1 - x, (0, 1, 2))

        @pl.when(mixes)
        def _():
            with scope("cwait"):
                for column in range(2):

                    @pl.when(zz * 2 + column != s)
                    def _():
                        c_arrival(zz * 2 + column).wait_recv()

            with scope("local"):
                local(zz * 2, zz * 2 + 1)

    def drain():
        wait_bytes(c_all.at[pl.ds(0, (n - 1) * rows)], c_sent)
        wait_bytes(w_all.at[pl.ds(0, (ny - 1) * depth)], w_sent.at[0])
        wait_bytes(w_all.at[pl.ds(0, ny * depth)], w_sent.at[1])
        if bridged:

            @pl.when(inner)
            def _():
                wait_bytes(c_via, v_sent)

        for zz in range(nz):
            lines = (zz + 1 if zz + 1 < nz else 0) + (nz - zz if zz else 0)
            sides = nz
            if bridged and 0 < zz < nz - 1:
                sides -= (zz == 1) + (zz == nz - 2)
            elif bridged:
                sides += 1

            @pl.when(z == zz)
            def _():
                wait_bytes(h_all.at[pl.ds(0, lines * rows)], h_sent.at[0])
                wait_bytes(h_all.at[pl.ds(0, sides * rows)], h_sent.at[1])

    return drain


def project_block(h_all, w_all, p_all, rows, columns, scale, block, which):
    at = pl.ds(pl.multiple_of(block * rows, rows), rows)
    for j in which:
        value = dot(h_all[at, :], w_all[:, j * columns : (j + 1) * columns]).astype(BF16)
        if j == 1:
            value = (value.astype(F32) * scale).astype(BF16)
        p_all[at, j * columns : (j + 1) * columns] = value


def fill_tables(heads, rate, inner, inner_t, query_decay, key_decay):
    dim = query_decay.shape[2]
    row = lax.broadcasted_iota(jnp.int32, (BLOCK, BLOCK), 0).astype(F32)
    col = lax.broadcasted_iota(jnp.int32, (BLOCK, BLOCK), 1).astype(F32)
    place = lax.broadcasted_iota(jnp.int32, (BLOCK, dim), 0).astype(F32)
    spread = row - col
    for h in range(heads):
        g = rate[h]
        inner[h] = jnp.where(spread >= 0, jnp.exp(g * jnp.maximum(spread, 0.0)), 0.0)
        inner_t[h] = jnp.where(spread <= 0, jnp.exp(g * jnp.maximum(-spread, 0.0)), 0.0)
        query_decay[h] = jnp.exp(g * (place + 1.0))
        key_decay[h] = jnp.exp(g * (BLOCK - 1.0 - place))


def head_parts(columns, dim, h):
    return [slice(j * columns + h * dim, j * columns + (h + 1) * dim) for j in range(3)]


def local_block(heads, c_all, p_all, inner, inner_t, query_decay, key_decay, acc, s_term, r_term, *blocks):
    columns = c_all.shape[1]
    dim = columns // heads
    for h, block in ((h, block) for h in range(heads) for block in blocks):
        at = pl.ds(pl.multiple_of(block * BLOCK, BLOCK), BLOCK)
        parts = head_parts(columns, dim, h)
        q, k, v = (p_all[at, part] for part in parts)
        c = c_all[at, parts[0]]
        mixed = (dot(c, v, NT) * inner[h]).astype(BF16)
        mixed_t = (dot(v, c, NT) * inner_t[h]).astype(BF16)
        scores_t = (dot(k, q, NT) * inner_t[h]).astype(BF16)
        s_term[block, h] = dot(v, (k.astype(F32) * key_decay[h]).astype(BF16), TN)
        r_term[block, h] = dot((q.astype(F32) * query_decay[h]).astype(BF16), c, TN)
        acc[at, parts[0]] = dot(mixed, k)
        acc[at, parts[1]] = dot(mixed_t, q)
        acc[at, parts[2]] = dot(scores_t, c)


def chain_phase(heads, rate, c_all, p_all, g_all, query_decay, key_decay, acc, s_term, r_term, state, back):
    length, columns = c_all.shape
    dim = columns // heads
    blocks = length // BLOCK
    scale = dim ** (-0.5)
    for i in range(blocks):
        for h in range(heads):
            block_decay = jnp.exp(jnp.full((1, dim), rate[h] * BLOCK, F32))
            parts = head_parts(columns, dim, h)

            at = slice(i * BLOCK, (i + 1) * BLOCK)
            grad_q = acc[at, parts[0]]
            if i:
                held = state[h]
                grad_q = grad_q + dot(c_all[at, parts[0]], held.astype(BF16)) * query_decay[h]
                state[h] = held * block_decay + s_term[i, h]
            else:
                state[h] = s_term[i, h]
            g_all[at, parts[0]] = grad_q.astype(BF16)

            j = blocks - 1 - i
            at = slice(j * BLOCK, (j + 1) * BLOCK)
            grad_k, grad_v = acc[at, parts[1]], acc[at, parts[2]]
            if i:
                held = back[h]
                held_bf = held.astype(BF16)
                grad_k = grad_k + dot(p_all[at, parts[2]], held_bf, NT) * key_decay[h]
                grad_v = grad_v + dot(p_all[at, parts[1]], held_bf) * key_decay[h]
                back[h] = held * block_decay + r_term[j, h]
            else:
                back[h] = r_term[j, h]
            g_all[at, parts[1]] = (grad_k * scale).astype(BF16)
            g_all[at, parts[2]] = grad_v.astype(BF16)


def scatter_phase(
    n, m, drain, h_all, w_all, g_all, dh, dq, dk, dv,
    part, ring, turned, near_out, near_in, far_out, far_in,
    r_send, r_recv, n_send, n_recv, f_send, f_recv,
):
    s = lax.axis_index("sp")
    d = lax.axis_index("dp")
    z, x = s // 2, s % 2
    y, core = d // 2, d % 2
    nz, ny = n // 2, m // 2
    rows, width = dh.shape
    depth, columns = dq.shape
    chunk = width // CHUNKS
    lanes = rows // 2
    mate = d + 1 - 2 * core
    me = x * (n - 1 - z) + (1 - x) * z

    def at_ring(p):
        p = (p + 2 * n) % n
        hi = p // nz
        return (hi * (n - 1 - p) + (1 - hi) * p) * 2 + hi

    def far(o):
        return ((y + o) % ny) * 2 + core

    right, left = at_ring(me + 1), at_ring(me - 1)

    def own(offset):
        return pl.multiple_of(at_ring(me + offset) * rows, rows)

    ready = set()

    def partial(q, *offsets):
        todo = [o % n for o in offsets if (q, o % n) not in ready]
        if not todo:
            return
        ready.update((q, o) for o in todo)
        bases = [own(o) for o in todo]
        with scope("partial", q, *todo):
            lhs = jnp.concatenate([g_all[pl.ds(base, rows), :] for base in bases], axis=0)
            value = dot(lhs, w_all[q * chunk : (q + 1) * chunk, :], NT).astype(BF16)
            for place, base in enumerate(bases):
                part[q, pl.ds(base, rows), :] = value[place * rows : (place + 1) * rows]

    def spot(way, piece):
        return way * (CHUNKS // 2) + piece // 2, (piece % 2) * lanes

    def r_copy(step, way, piece):
        q, lane = spot(way, piece)
        if step == 0:
            base = own(-1 if way == 0 else 1)
            src = part.at[q, pl.ds(pl.multiple_of(base + lane, lanes), lanes)]
        else:
            src = ring.at[step - 1, way, piece]
        return remote(
            src,
            ring.at[step, way, piece],
            r_send,
            r_recv.at[step, way, piece],
            {"sp": right if way == 0 else left},
        )

    def process(step, piece):
        for way in range(2):
            offset = -(step + 2) if way == 0 else step + 2
            q, lane = spot(way, piece)
            partial(q, -(step + 2), step + 2)
            with scope("ring", step, way, piece):
                r_copy(step, way, piece).wait_recv()
            mine = part[q, pl.ds(pl.multiple_of(own(offset) + lane, lanes), lanes), :]
            total = (ring[step, way, piece].astype(F32) + mine.astype(F32)).astype(BF16)
            if step < n - 2:
                ring[step, way, piece] = total
                r_copy(step + 1, way, piece).start()
            else:
                dh[lane : lane + lanes, q * chunk : (q + 1) * chunk] = total

    def turn(slot, device):
        turned[slot] = h_all[:, pl.ds(pl.multiple_of(device * depth, depth), depth)].T

    def weight_part(slot, j):
        return dot(turned[slot], g_all[:, j * columns : (j + 1) * columns])

    def n_copy(o, j):
        return remote(
            near_out.at[o, j], near_in.at[o, j], n_send, n_recv.at[o, j], {"dp": mate}
        )

    def f_copy(o, j):
        return remote(
            far_out.at[o - 1, j], far_in.at[o - 1, j], f_send, f_recv.at[o - 1, j], {"dp": far(o)}
        )

    def near(o, j):
        if j == 0:
            turn(0, far(o) + 1 - 2 * core)
        with scope("near", o, j):
            near_out[o, j] = weight_part(0, j).astype(BF16)
        n_copy(o, j).start()

    def chip_sum(o, j):
        if j == 0:
            turn(1, far(o))
        with scope("chip_sum", o, j):
            value = weight_part(1, j)
            n_copy(o, j).wait_recv()
            value = value + near_in[o, j].astype(F32)
        if o:
            far_out[o - 1, j] = value.astype(BF16)
            f_copy(o, j).start()
        else:
            (dq, dk, dv)[j][...] = value

    def weight(kind, o, j):
        return functools.partial(kind, o, j)

    tasks = []
    for o in list(range(1, ny)) + [0]:
        first = [weight(near, o, 0), weight(chip_sum, o, 0)]
        later = [weight(near, o, 1), weight(near, o, 2), weight(chip_sum, o, 1), weight(chip_sum, o, 2)]
        tasks += first + later if o else [first[0], *later[:2], first[1], *later[2:]]

    def work(count=1):
        for _ in range(count):
            if tasks:
                tasks.pop(0)()

    order = [q for k in range(CHUNKS // 2) for q in (k, CHUNKS // 2 + k)]
    for spot_in_order, q in enumerate(order):
        if spot_in_order == 2:
            work()
        partial(q, -1, 1)
        way, first = divmod(q, CHUNKS // 2)
        for piece in (2 * first, 2 * first + 1):
            r_copy(0, way, piece).start()
    partial(order[0], -2, 2)
    partial(order[1], -2, 2)
    work()
    pairs = [(q, pair) for pair in [(-2, 2), (-3, 3), (n // 2, 0)] for q in order]
    def finish_weight(j):
        out = (dq, dk, dv)[j]
        total = out[...]
        for o in range(1, ny):
            with scope("fwait", o, j):
                f_copy(o, j).wait_recv()
            total = total + far_in[o - 1, j].astype(F32)
        out[...] = total * (1.0 / m)

    def wait_bytes(ref, sem):
        pltpu.make_async_copy(ref, ref, sem).wait()

    def settle():
        wait_bytes(near_out, n_send)
        drain()

    for step in range(n - 1):
        for piece in range(PIECES):
            if step == n - 2 and piece != 2:
                finish_weight(min(piece, 2))
            if step == n - 3 and piece == 0:
                work(len(tasks))
                settle()
            process(step, piece)
            while pairs and all((pairs[0][0], o % n) in ready for o in pairs[0][1]):
                pairs.pop(0)
            if pairs and (step < 2 or not tasks):
                q, pair = pairs.pop(0)
                partial(q, *pair)
                if step and piece % 2:
                    work()
            else:
                work()
    with scope("tail"):
        wait_bytes(far_out, f_send)
        wait_bytes(ring, r_send)


def whole_kernel(n, m, heads, rate_in, h_in, c_in, wq, wk, wv, dh, dq, dk, dv, *scratch):
    rate, *scratch = scratch
    h_all, c_all, w_all, p_all, g_all, state, back = scratch[:7]
    decays, (acc, s_term, r_term) = scratch[7:11], scratch[11:14]
    gather_refs, rest = scratch[14:26], scratch[26:]
    columns = wq.shape[1]
    project = functools.partial(
        project_block, h_all, w_all, p_all, h_in.shape[0], columns, (columns // heads) ** (-0.5)
    )
    local = functools.partial(local_block, heads, c_all, p_all, *decays, acc, s_term, r_term)
    tables = functools.partial(fill_tables, heads, rate, *decays)
    drain = gather_phase(
        n, m, project, local, tables, rate_in, rate, h_in, c_in, wq, wk, wv, h_all, c_all, w_all,
        *gather_refs,
    )
    with scope("chain"):
        chain_phase(heads, rate, c_all, p_all, g_all, *decays[2:], acc, s_term, r_term, state, back)
    scatter_phase(n, m, drain, h_all, w_all, g_all, dh, dq, dk, dv, *rest)


def whole(n, m, rate, h, c, wq, wk, wv):
    rows, width = h.shape
    depth, columns = wq.shape
    heads = rate.shape[0]
    dim = columns // heads
    length = rows * n
    ny = m // 2
    vmem = pl.BlockSpec(memory_space=pltpu.VMEM)
    dma = pltpu.SemaphoreType.DMA
    return pl.pallas_call(
        functools.partial(whole_kernel, n, m, heads),
        out_shape=(pltpu.VMEM((rows, width), BF16),)
        + (pltpu.VMEM((depth, columns), F32),) * 3,
        in_specs=[pl.BlockSpec(memory_space=pl.ANY)] * 6,
        out_specs=(vmem,) * 4,
        scratch_shapes=[
            pltpu.SMEM((heads,), F32),
            pltpu.VMEM((length, width), BF16),
            pltpu.VMEM((length, columns), BF16),
            pltpu.VMEM((depth * m, 3 * columns), BF16),
            pltpu.VMEM((length, 3 * columns), BF16),
            pltpu.VMEM((length, 3 * columns), BF16),
            pltpu.VMEM((heads, dim, dim), F32),
            pltpu.VMEM((heads, dim, dim), F32),
            pltpu.VMEM((heads, BLOCK, BLOCK), F32),
            pltpu.VMEM((heads, BLOCK, BLOCK), F32),
            pltpu.VMEM((heads, BLOCK, dim), F32),
            pltpu.VMEM((heads, BLOCK, dim), F32),
            pltpu.VMEM((length, 3 * columns), F32),
            pltpu.VMEM((length // BLOCK, heads, dim, dim), F32),
            pltpu.VMEM((length // BLOCK, heads, dim, dim), F32),
            pltpu.VMEM((rows, columns * n), BF16),
            pltpu.VMEM((2, rows, columns), BF16),
            dma((7,)),
            dma((n, SUBS)),
            dma((2,)),
            dma(()),
            dma((n,)),
            dma(()),
            dma((2,)),
            dma((2,)),
            dma((3,)),
            dma((ny, 3)),
            pltpu.VMEM((CHUNKS, length, width // CHUNKS), BF16),
            pltpu.VMEM((n - 1, 2, PIECES, rows // 2, width // CHUNKS), BF16),
            pltpu.VMEM((2, depth, length), BF16),
            pltpu.VMEM((ny, 3, depth, columns), BF16),
            pltpu.VMEM((ny, 3, depth, columns), BF16),
            pltpu.VMEM((ny - 1, 3, depth, columns), BF16),
            pltpu.VMEM((ny - 1, 3, depth, columns), BF16),
            dma(()),
            dma((n - 1, 2, PIECES)),
            dma(()),
            dma((ny, 3)),
            dma(()),
            dma((ny - 1, 3)),
        ],
        compiler_params=pltpu.CompilerParams(
            collective_id=0, has_side_effects=True, vmem_limit_bytes=VMEM_LIMIT
        ),
        name="whole",
    )(rate, h, c, wq, wk, wv)


def finish_kernel(count, *refs):
    ins, outs, sems = refs[:count], refs[count : 2 * count], refs[2 * count]
    moves = [pltpu.make_async_copy(ins[i], outs[i], sems.at[i]) for i in range(count)]
    for move in moves:
        move.start()
    for move in moves:
        move.wait()


def finish(*arrays):
    count = len(arrays)
    return pl.pallas_call(
        functools.partial(finish_kernel, count),
        out_shape=tuple(jax.ShapeDtypeStruct(a.shape, a.dtype) for a in arrays),
        in_specs=[pl.BlockSpec(memory_space=pltpu.VMEM)] * count,
        out_specs=(pl.BlockSpec(memory_space=pl.ANY),) * count,
        scratch_shapes=[pltpu.SemaphoreType.DMA((count,))],
        compiler_params=pltpu.CompilerParams(vmem_limit_bytes=4 * 1024 * 1024),
        name="finish",
    )(*arrays)


def body(n, m, hidden_in, mix_cotangent, query_weight, key_weight, value_weight, decay_log):
    dh, dq, dk, dv = finish(
        *whole(
            n, m, decay_log, hidden_in[0], mix_cotangent[0], query_weight, key_weight, value_weight
        )
    )
    return dh[None], dq, dk, dv


def solution(mesh):
    placed = (
        P("dp", "sp", None),
        P("dp", "sp", None),
        P("dp", "sp"),
        P("dp", "sp"),
        P("dp", "sp"),
        P("sp"),
    )
    return jax.shard_map(
        functools.partial(body, mesh.shape["sp"], mesh.shape["dp"]),
        mesh=mesh,
        in_specs=placed,
        out_specs=(P("dp", "sp", None), P("dp", "sp"), P("dp", "sp"), P("dp", "sp")),
        check_vma=False,
    )
```

```python
import functools

import jax
import jax.numpy as jnp
from jax import lax
from jax.experimental import pallas as pl
from jax.experimental.pallas import tpu as pltpu
from jax.sharding import PartitionSpec as P

BLOCK = 128
SUBS = 2
CHUNKS = 4
PIECES = 4
F32 = jnp.float32
BF16 = jnp.bfloat16
MESH = pl.DeviceIdType.MESH
NT = (((1,), (1,)), ((), ()))
TN = (((0,), (0,)), ((), ()))
VMEM_LIMIT = 58 * 1024 * 1024


def dot(a, b, dims=(((1,), (0,)), ((), ()))):
    return lax.dot_general(a, b, dims, preferred_element_type=F32)


def scope(name, *tags):
    return jax.named_scope("#".join([name] + [str(t) for t in tags]))


def remote(src, dst, send, recv, where):
    return pltpu.make_async_remote_copy(
        src_ref=src, dst_ref=dst, send_sem=send, recv_sem=recv, device_id=where, device_id_type=MESH
    )


def greet(always, sometimes):
    barrier = pltpu.get_barrier_semaphore()
    count = len(always)
    for where in always:
        pl.semaphore_signal(barrier, inc=1, device_id=where, device_id_type=MESH)
    for there, where in sometimes:
        count = count + jnp.where(there, 1, 0)

        @pl.when(there)
        def _():
            pl.semaphore_signal(barrier, inc=1, device_id=where, device_id_type=MESH)

    return lambda: pl.semaphore_wait(barrier, count)


def gather_phase(
    n, m, project, local, tables, rate_in, rate, h_in, c_in, wq, wk, wv, h_all, c_all, w_all,
    c_own, c_via, l_sem,
    h_recv, h_sent, c_sent, c_recv, v_sent, v_recv, w_sent, w_near, w_recv,
):
    s = lax.axis_index("sp")
    d = lax.axis_index("dp")
    z, x = s // 2, s % 2
    y, core = d // 2, d % 2
    nz, ny = n // 2, m // 2
    rows = h_in.shape[0]
    sub_rows = rows // SUBS
    depth, columns = wq.shape
    side = s + 1 - 2 * x
    mate = d + 1 - 2 * core
    bridged = nz > 2
    is_end = jnp.logical_or(z == 0, z == nz - 1)
    inner = jnp.logical_not(is_end)
    inward = jnp.where(z == 0, s + 2, s - 2)

    def far(o):
        return ((y + o) % ny) * 2 + core

    def part_rows(block):
        return pl.ds(pl.multiple_of(block * rows, rows), rows)

    def part_columns(block):
        return pl.ds(pl.multiple_of(block * columns, columns), columns)

    own_depth = pl.ds(pl.multiple_of(d * depth, depth), depth)
    loads = [pltpu.make_async_copy(h_in, h_all.at[part_rows(s)], l_sem.at[0])]
    loads[0].start()
    arrived = greet(
        [{"sp": side}, {"dp": mate}] + [{"dp": far(o)} for o in range(1, ny)],
        [(z >= 1, {"sp": s - 2}), (z + 1 < nz, {"sp": s + 2})],
    )
    for j, w in enumerate((wq, wk, wv)):
        place = w_all.at[own_depth, pl.ds(j * columns, columns)]
        loads.append(pltpu.make_async_copy(w, place, l_sem.at[1 + j]))
    loads.append(pltpu.make_async_copy(c_in, c_own, l_sem.at[4]))
    mine = c_in.at[:, part_columns(s)]
    loads.append(pltpu.make_async_copy(mine, c_all.at[part_rows(s)], l_sem.at[5]))
    loads.append(pltpu.make_async_copy(rate_in, rate, l_sem.at[6]))
    for load in loads[1:]:
        load.start()

    def h_copy(src_z, src_x, sub, dest, send):
        block = src_z * 2 + src_x
        place = pl.ds(pl.multiple_of(block * rows + sub * sub_rows, sub_rows), sub_rows)
        return remote(h_all.at[place], h_all.at[place], send, h_recv.at[block, sub], {"sp": dest})

    def w_copy(src_d, j, dest, send, recv):
        place = w_all.at[
            pl.ds(pl.multiple_of(src_d * depth, depth), depth), pl.ds(j * columns, columns)
        ]
        return remote(place, place, send, recv, {"dp": dest})

    def w_far_copy(src_d, j, dest):
        return w_copy(src_d, j, dest, w_sent.at[0], w_recv.at[src_d // 2, j])

    def w_near_copy(src_d, j):
        return w_copy(src_d, j, mate, w_sent.at[1], w_near.at[j])

    def wait_bytes(ref, sem):
        pltpu.make_async_copy(ref, ref, sem).wait()

    def c_copy(to):
        return remote(
            c_own.at[:, part_columns(to)], c_all.at[part_rows(s)], c_sent, c_recv.at[s], {"sp": to}
        )

    def c_arrival(block):
        return remote(
            c_all.at[part_rows(block)], c_all.at[part_rows(block)], c_sent, c_recv.at[block], {"sp": side}
        )

    def end_block(e, column):
        return e * (nz - 1) * 2 + column

    def c_cross(e):
        to = end_block(e, 1 - x)
        return remote(
            c_own.at[:, part_columns(to)], c_via.at[e], c_sent, v_recv.at[e], {"sp": side}
        )

    def c_pass(e):
        return remote(
            c_via.at[e], c_all.at[part_rows(side)], v_sent, c_recv.at[side], {"sp": end_block(e, x)}
        )

    def line(k, sub, up):
        source = (z - k) if up else (z + k)
        dest = (s + 2) if up else (s - 2)
        return h_copy(source, x, sub, dest, h_sent.at[0])

    def goes(k, up):
        if up:
            return jnp.logical_and(z - k >= 0, z + 1 < nz)
        return jnp.logical_and(z + k < nz, z >= 1)

    def arrives(k, up):
        return (z - k >= 0) if up else (z + k < nz)

    def crosses(k, up):
        here = arrives(k, up)
        if not bridged or k != 1:
            return here
        return jnp.logical_and(here, (z != 1) if up else (z != nz - 2))

    def bridge(sub):
        return h_copy(z, 1 - x, sub, inward, h_sent.at[1])

    with scope("greet"):
        loads[0].wait()
        arrived()
    for sub in range(SUBS):
        for up in (True, False):

            @pl.when(goes(0, up))
            def _():
                line(0, sub, up).start()

        h_copy(z, x, sub, side, h_sent.at[1]).start()
    for j in range(3):
        loads[1 + j].wait()
        for o in range(1, ny):
            w_far_copy(d, j, far(o)).start()
        w_near_copy(d, j).start()
    loads[4].wait()
    loads[5].wait()
    if bridged:

        @pl.when(inner)
        def _():
            for e in range(2):
                c_cross(e).start()
            c_copy(side).start()

    loads[6].wait()
    tables()

    def pass_weights(j):
        for o in range(1, ny):
            with scope("wfar", j):
                w_far_copy(far(o), j, mate).wait_recv()
            w_near_copy(far(o), j).start()

    def send_level(k):
        for up in (True, False):
            to_z = (z + k) if up else (z - k)

            @pl.when((to_z < nz) if up else (to_z >= 0))
            def _():
                c_copy(to_z * 2 + x).start()
                c_copy(to_z * 2 + 1 - x).start()

    def send_column(k):
        for up in (True, False):
            to_z = (z + k) if up else (z - k)

            @pl.when((to_z < nz) if up else (to_z >= 0))
            def _():
                c_copy(to_z * 2 + x).start()

            @pl.when(to_z == (nz - 1 if up else 0))
            def _():
                c_cross(int(up)).wait_recv()
                c_pass(int(up)).start()

    def send_across(k):
        for up in (True, False):
            to_z = (z + k) if up else (z - k)

            @pl.when((to_z < nz - 1) if up else (to_z >= 1))
            def _():
                c_copy(to_z * 2 + 1 - x).start()

    upper = z // ((nz + 1) // 2)
    from_low = upper * (nz - 1) + (1 - 2 * upper) * z

    def level(k):
        low = jnp.where(k == 0, from_low, jnp.where(k - 1 < from_low, k - 1, k))
        return upper * (nz - 1) + (1 - 2 * upper) * low

    def side_wait(zz):
        fresh = jnp.logical_not(jnp.logical_and(is_end, zz == z)) if bridged else True
        with scope("sidewait"):

            @pl.when(fresh)
            def _():
                for sub in range(SUBS):
                    h_copy(zz, 1 - x, sub, side, h_sent.at[1]).wait_recv()

    def wait_weights(j):
        with scope("wmate", j):
            wait_bytes(w_all.at[pl.ds(0, ny * depth), pl.ds(j * columns, columns)], w_near.at[j])

    def early():
        for j in range(2):
            wait_weights(j)
        with scope("early"):

            @pl.loop(0, nz - 1)
            def _(k):
                project(level(k) * 2 + x, (0, 1))

            side_wait(level(0))
            project(level(0) * 2 + 1 - x, (0, 1))

    passed = 0
    for k in range(1, nz):
        if bridged and k == nz - 1:

            @pl.when(inner)
            def _():
                send_column(1)

        for sub in range(SUBS):
            for up in (True, False):

                @pl.when(arrives(k, up))
                def _():
                    source = (z - k) if up else (z + k)
                    with scope("hline", k, sub, up):
                        h_copy(source, x, sub, side, h_sent.at[1]).wait_recv()

                @pl.when(crosses(k, up))
                def _():
                    source = (z - k) if up else (z + k)
                    h_copy(source, x, sub, side, h_sent.at[1]).start()

                @pl.when(goes(k, up))
                def _():
                    line(k, sub, up).start()

            if bridged and k == 1:

                @pl.when(is_end)
                def _():
                    h_copy(z, 1 - x, sub, side, h_sent.at[1]).wait_recv()
                    bridge(sub).start()

            if bridged and (k, sub) in ((nz - 2, 0), (nz - 2, SUBS - 1), (nz - 1, 0)):
                if passed == 2:

                    @pl.when(is_end)
                    def _():
                        for past in range(2, nz - 1):
                            send_level(past)

                    early()
                pass_weights(passed)
                passed += 1
        if bridged and k == 1:

            @pl.when(is_end)
            def _():
                c_copy(side).start()
                send_level(1)

    if bridged:

        @pl.when(inner)
        def _():
            send_across(1)

    else:
        c_copy(side).start()
        for k in range(1, nz):
            send_level(k)

    for j in range(passed, 3):
        if j == 2:
            early()
        pass_weights(j)
    wait_weights(2)
    if bridged:

        @pl.when(inner)
        def _():
            for k in range(2, nz):
                send_column(k)
                send_across(k)

    @pl.loop(0, nz - 1)
    def _(k):
        project(level(k) * 2 + x, (2,))

    project(level(0) * 2 + 1 - x, (2,))
    project(level(nz - 1) * 2 + x, (0, 1, 2))

    @pl.loop(0, 2 * nz - 1)
    def _(t):
        inside = jnp.logical_and(t >= nz - 1, t < 2 * nz - 2)
        middle = jnp.logical_and(jnp.logical_and(is_end, inside), t != max(2 * nz - 4, 1))
        outer = jnp.logical_or(t == 0, t == 2 * nz - 2)
        mixes = jnp.where(is_end, jnp.logical_or(outer, middle), t % 2 == 0)
        at_end = jnp.where(t < nz - 1, t, nz - 1)
        zz = level(jnp.where(is_end, at_end, (t + 1) // 2))

        def unit(u):
            column = jnp.where(u < nz - 2, x, 1 - x)
            return level(1 + u % max(nz - 2, 1)) * 2 + column

        first = 2 * jnp.clip(t - (nz - 1), 0, max(nz - 3, 0))
        blocks = [
            jnp.where(middle, unit(first), zz * 2 + x),
            jnp.where(middle, unit(first + 1), zz * 2 + 1 - x),
        ]
        if bridged:

            @pl.when(jnp.logical_and(is_end, t == 1))
            def _():
                send_level(nz - 1)

        @pl.when(jnp.logical_not(mixes))
        def _():
            side_wait(zz)
            with scope("projside"):
                project(zz * 2 + 1 - x, (0, 1, 2))

        @pl.when(mixes)
        def _():
            with scope("cwait"):
                for block in blocks:

                    @pl.when(block != s)
                    def _():
                        c_arrival(block).wait_recv()

            with scope("local"):
                local(*blocks)

    def drain():
        wait_bytes(c_all.at[pl.ds(0, (n - 1) * rows)], c_sent)
        wait_bytes(w_all.at[pl.ds(0, (ny - 1) * depth)], w_sent.at[0])
        wait_bytes(w_all.at[pl.ds(0, ny * depth)], w_sent.at[1])
        if bridged:

            @pl.when(inner)
            def _():
                wait_bytes(c_via, v_sent)

        for zz in range(nz):
            lines = (zz + 1 if zz + 1 < nz else 0) + (nz - zz if zz else 0)
            sides = nz
            if bridged and 0 < zz < nz - 1:
                sides -= (zz == 1) + (zz == nz - 2)
            elif bridged:
                sides += 1

            @pl.when(z == zz)
            def _():
                wait_bytes(h_all.at[pl.ds(0, lines * rows)], h_sent.at[0])
                wait_bytes(h_all.at[pl.ds(0, sides * rows)], h_sent.at[1])

    return drain


def project_block(h_all, w_all, p_all, rows, columns, scale, block, which):
    at = pl.ds(pl.multiple_of(block * rows, rows), rows)
    for j in which:
        value = dot(h_all[at, :], w_all[:, j * columns : (j + 1) * columns]).astype(BF16)
        if j == 1:
            value = (value.astype(F32) * scale).astype(BF16)
        p_all[at, j * columns : (j + 1) * columns] = value


def fill_tables(heads, rate, inner, inner_t, query_decay, key_decay):
    dim = query_decay.shape[2]
    row = lax.broadcasted_iota(jnp.int32, (BLOCK, BLOCK), 0).astype(F32)
    col = lax.broadcasted_iota(jnp.int32, (BLOCK, BLOCK), 1).astype(F32)
    place = lax.broadcasted_iota(jnp.int32, (BLOCK, dim), 0).astype(F32)
    spread = row - col
    for h in range(heads):
        g = rate[h]
        inner[h] = jnp.where(spread >= 0, jnp.exp(g * jnp.maximum(spread, 0.0)), 0.0)
        inner_t[h] = jnp.where(spread <= 0, jnp.exp(g * jnp.maximum(-spread, 0.0)), 0.0)
        query_decay[h] = jnp.exp(g * (place + 1.0))
        key_decay[h] = jnp.exp(g * (BLOCK - 1.0 - place))


def head_parts(columns, dim, h):
    return [slice(j * columns + h * dim, j * columns + (h + 1) * dim) for j in range(3)]


def local_block(heads, c_all, p_all, inner, inner_t, query_decay, key_decay, acc, s_term, r_term, *blocks):
    columns = c_all.shape[1]
    dim = columns // heads
    for h, block in ((h, block) for h in range(heads) for block in blocks):
        at = pl.ds(pl.multiple_of(block * BLOCK, BLOCK), BLOCK)
        parts = head_parts(columns, dim, h)
        q, k, v = (p_all[at, part] for part in parts)
        c = c_all[at, parts[0]]
        mixed = (dot(c, v, NT) * inner[h]).astype(BF16)
        mixed_t = (dot(v, c, NT) * inner_t[h]).astype(BF16)
        scores_t = (dot(k, q, NT) * inner_t[h]).astype(BF16)
        s_term[block, h] = dot(v, (k.astype(F32) * key_decay[h]).astype(BF16), TN)
        r_term[block, h] = dot((q.astype(F32) * query_decay[h]).astype(BF16), c, TN)
        acc[at, parts[0]] = dot(mixed, k)
        acc[at, parts[1]] = dot(mixed_t, q)
        acc[at, parts[2]] = dot(scores_t, c)


def chain_phase(heads, rate, c_all, p_all, g_all, query_decay, key_decay, acc, s_term, r_term, state, back):
    length, columns = c_all.shape
    dim = columns // heads
    blocks = length // BLOCK
    scale = dim ** (-0.5)
    for i in range(blocks):
        for h in range(heads):
            block_decay = jnp.exp(jnp.full((1, dim), rate[h] * BLOCK, F32))
            parts = head_parts(columns, dim, h)

            at = slice(i * BLOCK, (i + 1) * BLOCK)
            grad_q = acc[at, parts[0]]
            if i:
                held = state[h]
                grad_q = grad_q + dot(c_all[at, parts[0]], held.astype(BF16)) * query_decay[h]
                state[h] = held * block_decay + s_term[i, h]
            else:
                state[h] = s_term[i, h]
            g_all[at, parts[0]] = grad_q.astype(BF16)

            j = blocks - 1 - i
            at = slice(j * BLOCK, (j + 1) * BLOCK)
            grad_k, grad_v = acc[at, parts[1]], acc[at, parts[2]]
            if i:
                held = back[h]
                held_bf = held.astype(BF16)
                grad_k = grad_k + dot(p_all[at, parts[2]], held_bf, NT) * key_decay[h]
                grad_v = grad_v + dot(p_all[at, parts[1]], held_bf) * key_decay[h]
                back[h] = held * block_decay + r_term[j, h]
            else:
                back[h] = r_term[j, h]
            g_all[at, parts[1]] = (grad_k * scale).astype(BF16)
            g_all[at, parts[2]] = grad_v.astype(BF16)


def scatter_phase(
    n, m, drain, h_all, w_all, g_all, dh, dq, dk, dv,
    part, ring, turned, near_out, near_in, far_out, far_in,
    r_send, r_recv, n_send, n_recv, f_send, f_recv,
):
    s = lax.axis_index("sp")
    d = lax.axis_index("dp")
    z, x = s // 2, s % 2
    y, core = d // 2, d % 2
    nz, ny = n // 2, m // 2
    rows, width = dh.shape
    depth, columns = dq.shape
    chunk = width // CHUNKS
    lanes = rows // 2
    mate = d + 1 - 2 * core
    me = x * (n - 1 - z) + (1 - x) * z

    def at_ring(p):
        p = (p + 2 * n) % n
        hi = p // nz
        return (hi * (n - 1 - p) + (1 - hi) * p) * 2 + hi

    def far(o):
        return ((y + o) % ny) * 2 + core

    right, left = at_ring(me + 1), at_ring(me - 1)

    def own(offset):
        return pl.multiple_of(at_ring(me + offset) * rows, rows)

    ready = set()

    def partial(q, *offsets):
        todo = [o % n for o in offsets if (q, o % n) not in ready]
        if not todo:
            return
        ready.update((q, o) for o in todo)
        bases = [own(o) for o in todo]
        with scope("partial", q, *todo):
            lhs = jnp.concatenate([g_all[pl.ds(base, rows), :] for base in bases], axis=0)
            value = dot(lhs, w_all[q * chunk : (q + 1) * chunk, :], NT).astype(BF16)
            for place, base in enumerate(bases):
                part[q, pl.ds(base, rows), :] = value[place * rows : (place + 1) * rows]

    def spot(way, piece):
        return way * (CHUNKS // 2) + piece // 2, (piece % 2) * lanes

    def r_copy(step, way, piece):
        q, lane = spot(way, piece)
        if step == 0:
            base = own(-1 if way == 0 else 1)
            src = part.at[q, pl.ds(pl.multiple_of(base + lane, lanes), lanes)]
        else:
            src = ring.at[step - 1, way, piece]
        return remote(
            src,
            ring.at[step, way, piece],
            r_send,
            r_recv.at[step, way, piece],
            {"sp": right if way == 0 else left},
        )

    def process(step, piece):
        for way in range(2):
            offset = -(step + 2) if way == 0 else step + 2
            q, lane = spot(way, piece)
            partial(q, -(step + 2), step + 2)
            with scope("ring", step, way, piece):
                r_copy(step, way, piece).wait_recv()
            mine = part[q, pl.ds(pl.multiple_of(own(offset) + lane, lanes), lanes), :]
            total = (ring[step, way, piece].astype(F32) + mine.astype(F32)).astype(BF16)
            if step < n - 2:
                ring[step, way, piece] = total
                r_copy(step + 1, way, piece).start()
            else:
                dh[lane : lane + lanes, q * chunk : (q + 1) * chunk] = total

    def turn(slot, device):
        turned[slot] = h_all[:, pl.ds(pl.multiple_of(device * depth, depth), depth)].T

    def weight_part(slot, j):
        return dot(turned[slot], g_all[:, j * columns : (j + 1) * columns])

    def n_copy(o, j):
        return remote(
            near_out.at[o, j], near_in.at[o, j], n_send, n_recv.at[o, j], {"dp": mate}
        )

    def f_copy(o, j):
        return remote(
            far_out.at[o - 1, j], far_in.at[o - 1, j], f_send, f_recv.at[o - 1, j], {"dp": far(o)}
        )

    def near(o, j):
        if j == 0:
            turn(0, far(o) + 1 - 2 * core)
        with scope("near", o, j):
            near_out[o, j] = weight_part(0, j).astype(BF16)
        n_copy(o, j).start()

    def chip_sum(o, j):
        if j == 0:
            turn(1, far(o))
        with scope("chip_sum", o, j):
            value = weight_part(1, j)
            n_copy(o, j).wait_recv()
            value = value + near_in[o, j].astype(F32)
        if o:
            far_out[o - 1, j] = value.astype(BF16)
            f_copy(o, j).start()
        else:
            (dq, dk, dv)[j][...] = value

    def weight(kind, o, j):
        return functools.partial(kind, o, j)

    tasks = []
    for o in list(range(1, ny)) + [0]:
        first = [weight(near, o, 0), weight(chip_sum, o, 0)]
        later = [weight(near, o, 1), weight(near, o, 2), weight(chip_sum, o, 1), weight(chip_sum, o, 2)]
        tasks += first + later if o else [first[0], *later[:2], first[1], *later[2:]]

    def work(count=1):
        for _ in range(count):
            if tasks:
                tasks.pop(0)()

    order = [q for k in range(CHUNKS // 2) for q in (k, CHUNKS // 2 + k)]
    for spot_in_order, q in enumerate(order):
        if spot_in_order == 2:
            work()
        partial(q, -1, 1)
        way, first = divmod(q, CHUNKS // 2)
        for piece in (2 * first, 2 * first + 1):
            r_copy(0, way, piece).start()
    partial(order[0], -2, 2)
    partial(order[1], -2, 2)
    work()
    pairs = [(q, pair) for pair in [(-2, 2), (-3, 3), (n // 2, 0)] for q in order]
    def finish_weight(j):
        out = (dq, dk, dv)[j]
        total = out[...]
        for o in range(1, ny):
            with scope("fwait", o, j):
                f_copy(o, j).wait_recv()
            total = total + far_in[o - 1, j].astype(F32)
        out[...] = total * (1.0 / m)

    def wait_bytes(ref, sem):
        pltpu.make_async_copy(ref, ref, sem).wait()

    def settle():
        wait_bytes(near_out, n_send)
        drain()

    for step in range(n - 1):
        for piece in range(PIECES):
            if step == n - 2 and piece != 2:
                finish_weight(min(piece, 2))
            if step == n - 3 and piece == 0:
                work(len(tasks))
                settle()
            process(step, piece)
            while pairs and all((pairs[0][0], o % n) in ready for o in pairs[0][1]):
                pairs.pop(0)
            if pairs and (step < 2 or not tasks):
                q, pair = pairs.pop(0)
                partial(q, *pair)
                if step and piece % 2:
                    work()
            else:
                work()
    with scope("tail"):
        wait_bytes(far_out, f_send)
        wait_bytes(ring, r_send)


def whole_kernel(n, m, heads, rate_in, h_in, c_in, wq, wk, wv, dh, dq, dk, dv, *scratch):
    rate, *scratch = scratch
    h_all, c_all, w_all, p_all, g_all, state, back = scratch[:7]
    decays, (acc, s_term, r_term) = scratch[7:11], scratch[11:14]
    gather_refs, rest = scratch[14:26], scratch[26:]
    columns = wq.shape[1]
    project = functools.partial(
        project_block, h_all, w_all, p_all, h_in.shape[0], columns, (columns // heads) ** (-0.5)
    )
    local = functools.partial(local_block, heads, c_all, p_all, *decays, acc, s_term, r_term)
    tables = functools.partial(fill_tables, heads, rate, *decays)
    drain = gather_phase(
        n, m, project, local, tables, rate_in, rate, h_in, c_in, wq, wk, wv, h_all, c_all, w_all,
        *gather_refs,
    )
    with scope("chain"):
        chain_phase(heads, rate, c_all, p_all, g_all, *decays[2:], acc, s_term, r_term, state, back)
    scatter_phase(n, m, drain, h_all, w_all, g_all, dh, dq, dk, dv, *rest)


def whole(n, m, rate, h, c, wq, wk, wv):
    rows, width = h.shape
    depth, columns = wq.shape
    heads = rate.shape[0]
    dim = columns // heads
    length = rows * n
    ny = m // 2
    vmem = pl.BlockSpec(memory_space=pltpu.VMEM)
    dma = pltpu.SemaphoreType.DMA
    return pl.pallas_call(
        functools.partial(whole_kernel, n, m, heads),
        out_shape=(pltpu.VMEM((rows, width), BF16),)
        + (pltpu.VMEM((depth, columns), F32),) * 3,
        in_specs=[pl.BlockSpec(memory_space=pl.ANY)] * 6,
        out_specs=(vmem,) * 4,
        scratch_shapes=[
            pltpu.SMEM((heads,), F32),
            pltpu.VMEM((length, width), BF16),
            pltpu.VMEM((length, columns), BF16),
            pltpu.VMEM((depth * m, 3 * columns), BF16),
            pltpu.VMEM((length, 3 * columns), BF16),
            pltpu.VMEM((length, 3 * columns), BF16),
            pltpu.VMEM((heads, dim, dim), F32),
            pltpu.VMEM((heads, dim, dim), F32),
            pltpu.VMEM((heads, BLOCK, BLOCK), F32),
            pltpu.VMEM((heads, BLOCK, BLOCK), F32),
            pltpu.VMEM((heads, BLOCK, dim), F32),
            pltpu.VMEM((heads, BLOCK, dim), F32),
            pltpu.VMEM((length, 3 * columns), F32),
            pltpu.VMEM((length // BLOCK, heads, dim, dim), F32),
            pltpu.VMEM((length // BLOCK, heads, dim, dim), F32),
            pltpu.VMEM((rows, columns * n), BF16),
            pltpu.VMEM((2, rows, columns), BF16),
            dma((7,)),
            dma((n, SUBS)),
            dma((2,)),
            dma(()),
            dma((n,)),
            dma(()),
            dma((2,)),
            dma((2,)),
            dma((3,)),
            dma((ny, 3)),
            pltpu.VMEM((CHUNKS, length, width // CHUNKS), BF16),
            pltpu.VMEM((n - 1, 2, PIECES, rows // 2, width // CHUNKS), BF16),
            pltpu.VMEM((2, depth, length), BF16),
            pltpu.VMEM((ny, 3, depth, columns), BF16),
            pltpu.VMEM((ny, 3, depth, columns), BF16),
            pltpu.VMEM((ny - 1, 3, depth, columns), BF16),
            pltpu.VMEM((ny - 1, 3, depth, columns), BF16),
            dma(()),
            dma((n - 1, 2, PIECES)),
            dma(()),
            dma((ny, 3)),
            dma(()),
            dma((ny - 1, 3)),
        ],
        compiler_params=pltpu.CompilerParams(
            collective_id=0, has_side_effects=True, vmem_limit_bytes=VMEM_LIMIT
        ),
        name="whole",
    )(rate, h, c, wq, wk, wv)


def finish_kernel(count, *refs):
    ins, outs, sems = refs[:count], refs[count : 2 * count], refs[2 * count]
    moves = [pltpu.make_async_copy(ins[i], outs[i], sems.at[i]) for i in range(count)]
    for move in moves:
        move.start()
    for move in moves:
        move.wait()


def finish(*arrays):
    count = len(arrays)
    return pl.pallas_call(
        functools.partial(finish_kernel, count),
        out_shape=tuple(jax.ShapeDtypeStruct(a.shape, a.dtype) for a in arrays),
        in_specs=[pl.BlockSpec(memory_space=pltpu.VMEM)] * count,
        out_specs=(pl.BlockSpec(memory_space=pl.ANY),) * count,
        scratch_shapes=[pltpu.SemaphoreType.DMA((count,))],
        compiler_params=pltpu.CompilerParams(vmem_limit_bytes=4 * 1024 * 1024),
        name="finish",
    )(*arrays)


def body(n, m, hidden_in, mix_cotangent, query_weight, key_weight, value_weight, decay_log):
    dh, dq, dk, dv = finish(
        *whole(
            n, m, decay_log, hidden_in[0], mix_cotangent[0], query_weight, key_weight, value_weight
        )
    )
    return dh[None], dq, dk, dv


def solution(mesh):
    placed = (
        P("dp", "sp", None),
        P("dp", "sp", None),
        P("dp", "sp"),
        P("dp", "sp"),
        P("dp", "sp"),
        P("sp"),
    )
    return jax.shard_map(
        functools.partial(body, mesh.shape["sp"], mesh.shape["dp"]),
        mesh=mesh,
        in_specs=placed,
        out_specs=(P("dp", "sp", None), P("dp", "sp"), P("dp", "sp"), P("dp", "sp")),
        check_vma=False,
    )
```
